32 devices in a mesh: sp: 8 (over z, core), tp: 4 (over y, x).
Axes of the slice: x: 2, y: 2, z: 4, core: 2. Of those that a mesh axis runs over, the one named last changes fastest.
Arguments:
- query_pairs: bfloat16 [2048, 2048], P('sp', 'tp'), may hold values from -8 to 8
- key_pairs: bfloat16 [2048, 2048], P('sp', 'tp'), may hold values from -6 to 6
- value_rows: bfloat16 [2048, 2048], P('sp', 'tp'), may hold values from -6 to 6
- doc_ids: int32 [2048], P('sp'), may hold values from 0 to 3, never falling along the last dimension, each value on 1 to 1280 neighbouring positions
- contrast_lambda: float32 [32], P('tp'), may hold values from 0.3 to 0.8
- head_gain: float32 [64], replicated, may hold values from 0.1 to 1.9
- stream: bfloat16 [2048, 2048], P('sp', 'tp'), may hold values from -6 to 6
- out_proj: bfloat16 [2048, 2048], P(None, 'tp'), may hold values from -0.125 to 0.125
- norm_gain: float32 [2048], replicated, may hold values from 0.1 to 1.9
- routes: int32 [2048, 2], P('sp'), may hold values from 0 to 7, all different within a row; in each aligned block of 256 rows (0 to 255, 256 to 511, ...) at most 128 rows name the same one
- route_weights: float32 [2048, 2], P('sp'), may hold values from 0.3 to 1.5
- expert_gate: bfloat16 [8, 2048, 2048], P('sp', None, 'tp'), may hold values from -0.125 to 0.125
- expert_up: bfloat16 [8, 2048, 2048], P('sp', None, 'tp'), may hold values from -0.125 to 0.125
- expert_down: bfloat16 [8, 2048, 2048], P('sp', None, 'tp'), may hold values from -0.125 to 0.125
- shared_gate: bfloat16 [2048, 2048], P(None, 'tp'), may hold values from -0.125 to 0.125
- shared_up: bfloat16 [2048, 2048], P(None, 'tp'), may hold values from -0.125 to 0.125
- shared_down: bfloat16 [2048, 2048], P(None, 'tp'), may hold values from -0.125 to 0.125
Outputs:
- mixed: bfloat16 [2048, 2048], P('sp', 'tp')
The draws below stay inside these ranges and needn't reach their ends.
Inputs may be any that keep to these rules, and one draw needn't show every extreme that they name: `doc_ids`: document numbers never fall along the positions; a document holds at most 1280 positions. `routes`: A position names 2 different experts. In each aligned block of 256 rows no expert is named by more than 128 rows, and every draw has a block in which some expert is named by exactly 128 rows.
All inputs are finite; a program needn't handle non-finite values.
Results may differ from the reference program's by a relative error of at most 0.011.
Values may be sent and summed in bfloat16 or wider, within the bound.
A program may use at most 64 MiB of HBM per device.

```python
import math
import jax
import jax.numpy as jnp
import numpy as np
from jax import lax

D = 2048
HEADS = 32
QK = 32
V = 64
FE = 2048
FS = 2048
TOP_K = 2
TOK_DEV = 256
TOKENS = 2048
EXPERTS = 8
CAP = 128
DOC_COUNT = 4
DOC_MOST = 1280
N_SP = 8


def paired_fields(key):
    base = jax.random.fold_in(key, 4321)
    query_seed, key_seed = jax.random.split(base, 2)
    shape = (TOKENS, HEADS, 2, QK)
    queries = jnp.clip(1.3 * jax.random.normal(query_seed, shape, jnp.float32), -6.0, 6.0)
    keys = jnp.clip(1.3 * jax.random.normal(key_seed, shape, jnp.float32), -6.0, 6.0)
    return (queries.reshape(TOKENS, HEADS * 2 * QK), keys.reshape(TOKENS, HEADS * 2 * QK))


def draw_query_pairs(key, part):
    return paired_fields(key)[0].astype(jnp.bfloat16)


def draw_key_pairs(key, part):
    return paired_fields(key)[1].astype(jnp.bfloat16)


def steps_of(rng, dims, cuts, low, high):
    loudness, own = 1.0, jax.random.fold_in(rng, 6)
    for axis_at, shards_of in cuts:
        draws = jnp.exp(jax.random.uniform(jax.random.fold_in(own, axis_at), (shards_of,), jnp.float32, low / len(cuts), high / len(cuts)))
        loudness = loudness * jnp.repeat(draws, dims[axis_at] // shards_of).reshape([-1 if axis == axis_at else 1 for axis in range(len(dims))])
    return loudness


def profile(count, total, most, lean):
    loads = [(1 << 20) // math.isqrt(rank ** lean) + 1 for rank in range(2, count + 1)]
    spare, holding = total - most - (count - 1), [1] * (count - 1)
    while spare > 0:
        free = [i for i in range(count - 1) if holding[i] < most]
        mass, remaining = sum([loads[i] for i in free]), spare
        for i in free:
            addition = min(most - holding[i], max(1, remaining * loads[i] // mass), spare)
            holding[i] = holding[i] + addition
            spare = spare - addition
    return np.array([most] + holding)


def uneven_parts(key, count, total, bound, skew):
    if count == 2:
        one = jax.random.randint(key, (), max(1, total - bound), min(bound, total - 1) + 1)
        return jnp.stack([one, total - one])
    sizes = jnp.asarray(profile(count, total, bound, skew), jnp.int32)
    pairs = (count - 1) // 2
    donor, receiver = sizes[1:1 + 2 * pairs:2], sizes[2:2 + 2 * pairs:2]
    slack = jnp.minimum(donor - 1, bound - receiver)
    shifted = jax.random.randint(jax.random.fold_in(key, 1), (pairs,), 0, 1 << 20) % (slack + 1)
    sizes = sizes.at[1:1 + 2 * pairs:2].set(donor - shifted).at[2:2 + 2 * pairs:2].set(receiver + shifted)
    return sizes[jax.random.permutation(jax.random.fold_in(key, 2), count)]


def assign_block(own_key, own, number, rows, number_of, top, most, lean):
    order = jax.random.permutation(own_key, number_of)
    crowded, ordinary = shares(number_of, rows * top, most, lean, True), shares(number_of, rows * top, most, lean, False)
    places = jnp.arange(number_of)

    def named(lengths, turn):
        used = int((lengths > 0).sum())
        fixed = max(1, used // 4)
        moved = fixed + (places - fixed + turn * (used - fixed)) % max(1, number_of - fixed)
        return jnp.zeros((number_of,), jnp.int32).at[order[jnp.where(places < fixed, places, moved)]].set(jnp.asarray(lengths, jnp.int32))

    lengths = jnp.where(number % 4 == 0, named(crowded, number // 4), named(ordinary, number - number // 4 - 1))
    mixed = jax.random.permutation(jax.random.fold_in(own, 3), number_of)
    donor, taker = mixed[0:number_of // 2 * 2:2], mixed[1:number_of // 2 * 2:2]
    margin = jnp.minimum(lengths[donor] - 1, most - lengths[taker]) // 2
    margin = jnp.where((donor == order[0]) | (taker == order[0]) | (lengths[taker] == 0), 0, jnp.maximum(margin, 0))
    moved = jax.random.randint(jax.random.fold_in(own, 4), (number_of // 2,), 0, 1 << 20) % (margin + 1)
    lengths = lengths.at[donor].add(-moved).at[taker].add(moved)
    members = jnp.searchsorted(jnp.cumsum(lengths), jnp.arange(rows * top), side="right").astype(jnp.int32)
    grid = members.reshape(top, rows).T
    grid = grid[jax.random.permutation(jax.random.fold_in(own, 1), rows)]
    turn = jax.random.randint(jax.random.fold_in(own, 2), (rows, 1), 0, top)
    return jnp.take_along_axis(grid, (jnp.arange(top)[None, :] + turn) % top, axis=1)


def shares(count, total, reach, lean, full):
    loads = [(1 << 20) // math.isqrt(grade ** lean) + 1 for grade in range(1, count + 1)]
    largest = reach if full else min(reach, max(-(-total // count), total * loads[0] // sum(loads)))
    least = 1 if total - largest >= count - 1 else 0
    given, spare = [largest] + [least] * (count - 1), total - largest - least * (count - 1)
    while spare > 0:
        candidates = [i for i in range(1, count) if given[i] < largest] or [i for i in range(1, count) if given[i] < reach]
        mass, left = sum([loads[i] for i in candidates]), spare
        for i in candidates:
            extra = min(reach - given[i], max(1, left * loads[i] // mass), spare)
            given[i] = given[i] + extra
            spare = spare - extra
    return np.array(given)


def bell_draw(rng, dims, deviation, reach, pieces=(), kind=jnp.bfloat16):
    entries = deviation * jax.random.normal(rng, dims, jnp.float32)
    if pieces:
        entries = entries * steps_of(rng, dims, pieces, -0.22, 0.18)
    return jnp.clip(entries, -reach, reach).astype(kind)


def setup_inputs(seed: int = 0) -> dict:
    splits = jax.random.split(jax.random.key(seed), 18)
    query_pairs = draw_query_pairs(jax.random.fold_in(splits[17], 71), 0)
    key_pairs = draw_key_pairs(jax.random.fold_in(splits[17], 71), 0)
    value_rows = bell_draw(splits[2], (TOKENS, HEADS * V), 1.0, 6.0, ((0, 8), (1, 4)))
    doc_ids = jnp.searchsorted(jnp.cumsum(uneven_parts(splits[3], DOC_COUNT, TOKENS, DOC_MOST, 1)), jnp.arange(TOKENS), side="right").astype(jnp.int32)
    contrast_lambda = jnp.clip(0.3 + 0.5 * jax.random.uniform(splits[4], (HEADS,), jnp.float32) ** steps_of(splits[4], (HEADS,), ((0, 4),), -0.2, 0.2), 0.3, 0.8)
    head_gain = jnp.clip(1.0 + 0.18 * jax.random.normal(splits[5], (V,), jnp.float32), 0.1, 1.9)
    stream = bell_draw(splits[6], (TOKENS, D), 1.0, 6.0, ((0, 8), (1, 4)))
    out_proj = bell_draw(splits[7], (HEADS * V, D), (HEADS * V) ** -0.5, 0.125, ((1, 4),))
    norm_gain = jnp.clip(1.0 + 0.18 * jax.random.normal(splits[8], (D,), jnp.float32), 0.1, 1.9)
    routes_keys = jax.random.split(jax.random.fold_in(splits[9], 1), TOKENS // TOK_DEV)
    routes_turns = jax.random.permutation(jax.random.fold_in(splits[9], 3), TOKENS // TOK_DEV)
    routes = jax.vmap(lambda own, number: assign_block(jax.random.fold_in(splits[9], 2), own, number, TOK_DEV, EXPERTS, TOP_K, CAP, 2))(routes_keys, routes_turns).reshape((TOKENS, TOP_K))
    route_weights = jnp.clip(0.3 + 1.2 * jax.random.uniform(splits[10], (TOKENS, TOP_K), jnp.float32) ** steps_of(splits[10], (TOKENS, TOP_K), ((0, 8),), -0.2, 0.2), 0.3, 1.5)
    expert_gate = bell_draw(splits[11], (EXPERTS, D, FE), D ** -0.5, 0.125, ((0, 8), (2, 4)))
    expert_up = bell_draw(splits[12], (EXPERTS, D, FE), D ** -0.5, 0.125, ((0, 8), (2, 4)))
    expert_down = bell_draw(splits[13], (EXPERTS, FE, D), FE ** -0.5, 0.125, ((0, 8), (2, 4)))
    shared_gate = bell_draw(splits[14], (D, FS), D ** -0.5, 0.125, ((1, 4),))
    shared_up = bell_draw(splits[15], (D, FS), D ** -0.5, 0.125, ((1, 4),))
    shared_down = bell_draw(splits[16], (FS, D), FS ** -0.5, 0.125, ((1, 4),))
    return {"query_pairs": query_pairs, "key_pairs": key_pairs, "value_rows": value_rows, "doc_ids": doc_ids, "contrast_lambda": contrast_lambda, "head_gain": head_gain, "stream": stream, "out_proj": out_proj, "norm_gain": norm_gain, "routes": routes, "route_weights": route_weights, "expert_gate": expert_gate, "expert_up": expert_up, "expert_down": expert_down, "shared_gate": shared_gate, "shared_up": shared_up, "shared_down": shared_down}


epsilon = 1e-06
floor_score = -1e+30

def attend(query_pairs, key_pairs, value_rows, doc_ids, contrast_lambda, head_gain):
    query_heads = jnp.transpose(query_pairs.reshape(TOKENS, HEADS, 2, QK), (1, 0, 2, 3)).astype(jnp.float32)
    key_heads = jnp.transpose(key_pairs.reshape(TOKENS, HEADS, 2, QK), (1, 0, 2, 3)).astype(jnp.float32)
    value_heads = jnp.transpose(value_rows.reshape(TOKENS, HEADS, V), (1, 0, 2)).astype(jnp.float32)
    positions = jnp.arange(TOKENS, dtype=jnp.int32)
    block_starts = jnp.arange(TOKENS // TOK_DEV, dtype=jnp.int32) * TOK_DEV

    def one_head(operands):
        queries, keys, values, weight = operands

        def one_block(block_start):
            block_query = lax.dynamic_slice_in_dim(queries, block_start, TOK_DEV, 0)
            block_pos = lax.dynamic_slice_in_dim(positions, block_start, TOK_DEV, 0)
            block_doc = lax.dynamic_slice_in_dim(doc_ids, block_start, TOK_DEV, 0)
            allowed = (positions[None, :] <= block_pos[:, None]) & (doc_ids[None, :] == block_doc[:, None])
            scores = jnp.einsum('qmd,kmd->mqk', block_query, keys) * QK ** (-0.5)
            scores = jnp.where(allowed, scores, floor_score)
            row_peak = lax.optimization_barrier(jnp.max(scores, axis=-1, keepdims=True))
            weights = jnp.where(allowed, jnp.exp(scores - row_peak), 0.0)
            rounded = lax.optimization_barrier(weights.astype(jnp.bfloat16)).astype(jnp.float32)
            heard = jnp.einsum('mqk,kv->mqv', rounded, values) / lax.optimization_barrier(jnp.sum(weights, axis=-1))[..., None]
            contrast = heard[0] - weight * heard[1]
            contrast = contrast * lax.rsqrt(lax.optimization_barrier(jnp.mean(contrast * contrast, axis=-1, keepdims=True)) + epsilon) * head_gain
            return contrast.astype(jnp.bfloat16)
        return lax.map(one_block, block_starts).reshape(TOKENS, V)
    heads = lax.map(one_head, (query_heads, key_heads, value_heads, contrast_lambda))
    return jnp.transpose(heads, (1, 0, 2)).reshape(TOKENS, HEADS * V)

def reference(query_pairs, key_pairs, value_rows, doc_ids, contrast_lambda, head_gain, stream, out_proj, norm_gain, routes, route_weights, expert_gate, expert_up, expert_down, shared_gate, shared_up, shared_down):
    head_out = attend(query_pairs, key_pairs, value_rows, doc_ids, contrast_lambda, head_gain)
    hidden_state = (stream.astype(jnp.float32) + jnp.dot(head_out, out_proj, preferred_element_type=jnp.float32)).astype(jnp.bfloat16)
    widened = hidden_state.astype(jnp.float32)
    normed = (widened * lax.rsqrt(lax.optimization_barrier(jnp.mean(widened * widened, axis=-1, keepdims=True)) + epsilon) * norm_gain).astype(jnp.bfloat16)
    shared_act = (jax.nn.silu(jnp.dot(normed, shared_gate, preferred_element_type=jnp.float32)) * jnp.dot(normed, shared_up, preferred_element_type=jnp.float32)).astype(jnp.bfloat16)
    shared_part = jnp.dot(shared_act, shared_down, preferred_element_type=jnp.float32)
    most_rows = N_SP * CAP

    def one_expert(running, operands):
        gate_weight, up_weight, down_weight, expert = operands
        matches = routes == expert
        picked = jnp.any(matches, axis=1)
        portion = lax.optimization_barrier(jnp.sum(jnp.where(matches, route_weights, 0.0), axis=1))
        chosen = jnp.nonzero(picked, size=most_rows, fill_value=0)[0].astype(jnp.int32)
        live = (jnp.arange(most_rows, dtype=jnp.int32) < jnp.sum(picked.astype(jnp.int32))).astype(jnp.float32)
        inputs = normed[chosen]
        expert_act = (jax.nn.silu(jnp.dot(inputs, gate_weight, preferred_element_type=jnp.float32)) * jnp.dot(inputs, up_weight, preferred_element_type=jnp.float32)).astype(jnp.bfloat16)
        expert_out = jnp.dot(expert_act, down_weight, preferred_element_type=jnp.float32).astype(jnp.bfloat16)
        scaled = expert_out.astype(jnp.float32) * (portion[chosen] * live)[:, None]
        return (running.at[chosen].add(scaled), None)
    routed, _ = lax.scan(one_expert, jnp.zeros((TOKENS, D), jnp.float32), (expert_gate, expert_up, expert_down, jnp.arange(EXPERTS, dtype=jnp.int32)))
    return (widened + shared_part + routed).astype(jnp.bfloat16)
```

```python
import functools
import math

import jax
import jax.numpy as jnp
from jax import lax
from jax.experimental import pallas as pl
from jax.experimental.pallas import tpu as pltpu
from jax.sharding import PartitionSpec as P

epsilon = 1e-06
floor_score = -1e30


def add_columns(weight_rows, part_block):
    return jnp.dot(part_block, weight_rows, preferred_element_type=jnp.float32)


def shards(
    query_pairs,
    key_pairs,
    value_rows,
    doc_ids,
    contrast_lambda,
    head_gain,
    stream,
    out_proj,
    norm_gain,
    routes,
    route_weights,
    expert_gate,
    expert_up,
    expert_down,
    shared_gate,
    shared_up,
    shared_down,
):
    row_count = query_pairs.shape[0]
    local_heads = contrast_lambda.shape[0]
    key_width = query_pairs.shape[1] // (2 * local_heads)
    value_width = value_rows.shape[1] // local_heads
    scaling = key_width ** (-0.5)
    first_row = lax.axis_index("sp") * row_count
    query_pos = first_row + jnp.arange(row_count, dtype=jnp.int32)
    last_query = first_row + row_count - 1
    first_doc = doc_ids[0]
    query_split = query_pairs.reshape(row_count, local_heads, 2, key_width)

    def absorb_block(running, key_block, value_block, doc_block, key_start):
        best, denom, numer = running
        span_len = key_block.shape[0]
        key_pos = key_start + jnp.arange(span_len, dtype=jnp.int32)
        allowed = (key_pos[None, :] <= query_pos[:, None]) & (
            doc_block[None, :] == doc_ids[:, None]
        )
        scores = (
            jnp.einsum(
                "qhmd,khmd->hmqk",
                query_split,
                key_block.reshape(span_len, local_heads, 2, key_width),
                preferred_element_type=jnp.float32,
            )
            * scaling
        )
        scores = jnp.where(allowed, scores, floor_score)
        new_best = jnp.maximum(best, jnp.max(scores, axis=-1))
        weights = jnp.where(allowed, jnp.exp(scores - new_best[..., None]), 0.0)
        fade = jnp.exp(best - new_best)
        denom = denom * fade + jnp.sum(weights, axis=-1)
        numer = numer * fade[..., None] + jnp.einsum(
            "hmqk,khv->hmqv",
            weights.astype(jnp.bfloat16),
            value_block.reshape(span_len, local_heads, value_width),
            preferred_element_type=jnp.float32,
        )
        return (new_best, denom, numer)

    start_best = jnp.full((local_heads, 2, row_count), floor_score, jnp.float32)
    start_denom = jnp.zeros((local_heads, 2, row_count), jnp.float32)
    start_numer = jnp.zeros((local_heads, 2, row_count, value_width), jnp.float32)
    key_piece = lax.all_gather(key_pairs, "sp", axis=0, tiled=True)
    value_piece = lax.all_gather(value_rows, "sp", axis=0, tiled=True)
    doc_piece = lax.all_gather(doc_ids, "sp", axis=0, tiled=True)
    length = key_piece.shape[0]
    span_len = row_count * max(1, 512 // row_count)

    def one_span(span_index, carried):
        offset = span_index * span_len
        key_block = lax.dynamic_slice_in_dim(key_piece, offset, span_len, 0)
        value_block = lax.dynamic_slice_in_dim(value_piece, offset, span_len, 0)
        doc_block = lax.dynamic_slice_in_dim(doc_piece, offset, span_len, 0)
        needed = (offset <= last_query) & (doc_block[span_len - 1] >= first_doc)
        return lax.cond(
            needed,
            lambda held: absorb_block(held, key_block, value_block, doc_block, offset),
            lambda held: held,
            carried,
        )

    best, denom, numer = lax.fori_loop(
        0, length // span_len, one_span, (start_best, start_denom, start_numer)
    )
    heard = numer / denom[..., None]
    contrast = heard[:, 0] - contrast_lambda[:, None, None] * heard[:, 1]
    contrast = (
        contrast
        * lax.rsqrt(jnp.mean(contrast * contrast, axis=-1, keepdims=True) + epsilon)
        * head_gain
    )
    head_out = (
        jnp.transpose(contrast, (1, 0, 2))
        .reshape(row_count, local_heads * value_width)
        .astype(jnp.bfloat16)
    )
    projected = add_columns(out_proj, lax.all_gather(head_out, "tp", axis=1, tiled=True))
    hidden_cols = (stream.astype(jnp.float32) + projected).astype(jnp.bfloat16)
    hidden_rows = lax.all_gather(hidden_cols, "tp", axis=1, tiled=True)
    widened = hidden_rows.astype(jnp.float32)
    normed = (
        widened
        * lax.rsqrt(jnp.mean(widened * widened, axis=-1, keepdims=True) + epsilon)
        * norm_gain
    ).astype(jnp.bfloat16)
    shared_act = (
        jax.nn.silu(jnp.dot(normed, shared_gate, preferred_element_type=jnp.float32))
        * jnp.dot(normed, shared_up, preferred_element_type=jnp.float32)
    ).astype(jnp.bfloat16)
    shared_cols = add_columns(shared_down, lax.all_gather(shared_act, "tp", axis=1, tiled=True))
    expert_count = lax.axis_size("sp")
    route_count = routes.shape[1]
    capacity = 2 * row_count * route_count // expert_count
    flat_routes = routes.reshape(-1)
    hits = (flat_routes[:, None] == jnp.arange(expert_count, dtype=jnp.int32)[None, :]).astype(
        jnp.int32
    )
    position = jnp.sum(jnp.cumsum(hits, axis=0) * hits, axis=1) - 1
    target = flat_routes * capacity + position
    sources = jnp.arange(flat_routes.shape[0], dtype=jnp.int32) // route_count
    owner = jnp.zeros((expert_count * capacity,), jnp.int32).at[target].set(sources)
    outgoing = normed[owner].reshape(expert_count, capacity, normed.shape[1])
    gate_cols = expert_gate[0]
    up_cols = expert_up[0]
    down_cols = expert_down[0]
    slice_width = outgoing.shape[2] // lax.axis_size("tp")
    own_slice = lax.dynamic_slice_in_dim(
        outgoing, lax.axis_index("tp") * slice_width, slice_width, 2
    )
    arrived = lax.all_to_all(own_slice, "sp", split_axis=0, concat_axis=0, tiled=True)
    apply_arrived = lax.all_gather(arrived, "tp", axis=2, tiled=True)
    gated = jnp.einsum("snd,df->snf", apply_arrived, gate_cols, preferred_element_type=jnp.float32)
    lifted = jnp.einsum("snd,df->snf", apply_arrived, up_cols, preferred_element_type=jnp.float32)
    expert_act = (jax.nn.silu(gated) * lifted).astype(jnp.bfloat16)
    expert_out = add_columns(
        down_cols, lax.all_gather(expert_act, "tp", axis=2, tiled=True)
    ).astype(jnp.bfloat16)
    returned = lax.all_to_all(expert_out, "sp", split_axis=0, concat_axis=0, tiled=True)
    flat_back = returned.reshape(expert_count * capacity, returned.shape[2])
    picked = (
        flat_back[target].reshape(row_count, route_count, returned.shape[2]).astype(jnp.float32)
    )
    routed = jnp.sum(picked * route_weights[:, :, None], axis=1)
    return (hidden_cols.astype(jnp.float32) + shared_cols + routed).astype(jnp.bfloat16)


MESH_ID = pl.DeviceIdType.MESH
VMEM = pl.BlockSpec(memory_space=pltpu.VMEM)
ANY = pl.BlockSpec(memory_space=pl.ANY)
SMEM = pl.BlockSpec(memory_space=pltpu.SMEM)


def flip(index, mask, size):
    out, bit = 0, 1
    while bit < size:
        out = out + bit * lax.rem(lax.div(index, bit) + lax.div(mask, bit), 2)
        bit *= 2
    return out


def remote(src, dst, send, recv, device):
    return pltpu.make_async_remote_copy(
        src_ref=src,
        dst_ref=dst,
        send_sem=send,
        recv_sem=recv,
        device_id=device,
        device_id_type=MESH_ID,
    )


def greet(devices):
    barrier = pltpu.get_barrier_semaphore()
    for device in devices:
        pl.semaphore_signal(barrier, inc=1, device_id=device, device_id_type=MESH_ID)
    pl.semaphore_wait(barrier, len(devices))


def fold_axes(me, col):
    core = lax.rem(me, 2)
    return flip(col, 2 - core, 4), flip(col, 1 + core, 4), flip(col, jnp.int32(3), 4)


def spread_kernel(
    count,
    width,
    q_ref,
    k_ref,
    v_ref,
    doc_ref,
    down_hbm,
    sdown_hbm,
    out_ref,
    docs_ref,
    down_out,
    sdown_out,
    pack,
    send,
    recv,
    dsend,
    drecv,
    wsend,
    wrecv,
):
    me, col = lax.axis_index("sp"), lax.axis_index("tp")
    rows = q_ref.shape[0]
    half = rows // 2
    peers = [(flip(me, jnp.int32(k), count), col) for k in range(count)]
    _, fold, across = fold_axes(me, col)
    swaps = [
        remote(src.at[quarter], dst.at[i], wsend.at[j, i], wrecv.at[j, i], (me, fold))
        for j, (src, dst) in enumerate(((down_hbm, down_out), (sdown_hbm, sdown_out)))
        for i, quarter in enumerate((fold, across))
    ]
    for h in range(count):
        cut = slice(h * width, (h + 1) * width)
        pack[h, :rows, :] = jnp.concatenate([q_ref[:, cut], k_ref[:, cut]], axis=1)
        pack[h, rows:, :] = jnp.concatenate([v_ref[:half, cut], v_ref[half:, cut]], axis=1)
    greet(peers[1:] + [(me, fold)])
    copies = []
    for k in reversed(range(1, count)):
        there = peers[k]
        copies.append(remote(doc_ref, docs_ref.at[me], dsend.at[k], drecv.at[k], there))
        copies.append(remote(pack.at[there[0]], out_ref.at[me], send.at[k], recv.at[k], there))
        copies[-2].start()
        copies[-1].start()
    for swap in swaps:
        swap.start()
    out_ref[me] = pack[me]
    docs_ref[me] = doc_ref[...]
    for copy in copies + swaps:
        copy.wait()


def attend_kernel(
    scaling, lam_ref, qkv_ref, doc_ref, gain_ref, out_ref, turned
):
    count, rows = doc_ref.shape[0], doc_ref.shape[2]
    half = rows // 2
    width = gain_ref.shape[1]
    weight = lam_ref[lax.axis_index("sp")]
    gains = jnp.concatenate([gain_ref[...], gain_ref[...]], axis=1)
    doc_rows = jnp.concatenate([doc_ref[b] for b in range(count)], axis=0).astype(jnp.float32)
    doc_cols = jnp.transpose(doc_rows)
    key_width = width // 2
    lanes = lax.broadcasted_iota(jnp.int32, (rows, 2 * width), 1)
    factor = scaling * math.log2(math.e)

    @pl.loop(0, count)
    def _(b):
        turned[b] = jnp.transpose(qkv_ref[b, rows:, :].astype(jnp.float32)).astype(jnp.bfloat16)

    @pl.loop(0, count)
    def _(b):
        moved = pltpu.roll(qkv_ref[b, :rows, :].astype(jnp.float32), width, 1)
        queries = [
            jnp.where(
                (lanes >= width + m * key_width) & (lanes < width + (m + 1) * key_width),
                moved,
                0.0,
            ).astype(jnp.bfloat16)
            for m in range(2)
        ]
        own_docs = doc_ref[b].astype(jnp.float32)
        earlier = jnp.zeros((rows, rows), jnp.float32)
        for kb in range(count):
            earlier = earlier + jnp.where(doc_cols[:, kb : kb + 1] < own_docs, 1.0, 0.0)
        earlier = jnp.sum(earlier, axis=0, keepdims=True)
        starts = earlier.astype(jnp.int32)
        first = lax.div(jnp.min(earlier).astype(jnp.int32), rows)
        query_pos = b * rows + lax.broadcasted_iota(jnp.int32, (1, rows), 1)

        def step(i, carried):
            tiles = []
            for part in range(2):
                kb = b - 2 * i - part
                key_pos = kb * rows + lax.broadcasted_iota(jnp.int32, (rows, rows), 0)
                allowed = (key_pos <= query_pos) & (key_pos >= starts)
                tiles.append((jnp.maximum(kb, 0), allowed))
            scores = [
                [
                    jnp.where(
                        allowed,
                        lax.dot_general(
                            qkv_ref[kb, :rows, :], queries[m], (((1,), (1,)), ((), ())),
                            preferred_element_type=jnp.float32,
                        )
                        * factor,
                        floor_score,
                    )
                    for kb, allowed in tiles
                ]
                for m in range(2)
            ]
            out = []
            for m in range(2):
                best, denom, numer = carried[m]
                tallest = jnp.max(jnp.maximum(*scores[m]), axis=0, keepdims=True)
                new_best = jnp.maximum(best, tallest)
                fade = jnp.exp2(best - new_best)
                weights = [jnp.exp2(tile - new_best) for tile in scores[m]]
                denom = denom * fade + jnp.sum(weights[0] + weights[1], axis=0, keepdims=True)
                numer = numer * fade
                for (kb, _), tile in zip(tiles, weights):
                    rounded = tile.astype(jnp.bfloat16)
                    numer = (
                        numer
                        + jnp.dot(
                            turned[kb, :width, :], rounded[:half],
                            preferred_element_type=jnp.float32,
                        )
                        + jnp.dot(
                            turned[kb, width:, :], rounded[half:],
                            preferred_element_type=jnp.float32,
                        )
                    )
                out.append((new_best, denom, numer))
            return tuple(out)

        begin = tuple(
            (
                jnp.full((1, rows), floor_score, jnp.float32),
                jnp.zeros((1, rows), jnp.float32),
                jnp.zeros((width, rows), jnp.float32),
            )
            for _ in range(2)
        )
        done = lax.fori_loop(0, lax.div(b - first, 2) + 1, step, begin)
        heard = [numer / denom for _, denom, numer in done]
        contrast = heard[0] - weight * heard[1]
        contrast = contrast * lax.rsqrt(
            jnp.mean(contrast * contrast, axis=0, keepdims=True) + epsilon
        )
        stacked = jnp.concatenate([contrast[:, :half], contrast[:, half:]], axis=0)
        out_ref[b] = (jnp.transpose(stacked) * gains).astype(jnp.bfloat16)


def layer_kernel(
    count,
    capacity,
    heads_ref,
    stream_ref,
    gain_ref,
    routes_ref,
    weight_ref,
    proj_hbm,
    sgate_hbm,
    sup_hbm,
    gate_hbm,
    up_hbm,
    sdown_hbm,
    down_hbm,
    sdown_far_hbm,
    down_far_hbm,
    out_ref,
    proj,
    sgate,
    sup,
    gate,
    up,
    sdown,
    down,
    held,
    head_buf,
    hidden_buf,
    normed,
    shared_buf,
    shared_part,
    onehot,
    outgoing,
    rows_in,
    acts,
    parts,
    kept,
    made,
    back,
    shared_cols,
    load_sem,
    hsend,
    hrecv,
    gsend,
    grecv,
    fsend,
    frecv,
    zsend,
    zrecv,
    rsend,
    rrecv,
):
    me, col = lax.axis_index("sp"), lax.axis_index("tp")
    rows, cols = stream_ref.shape
    half = rows // 2
    width = heads_ref.shape[2] // 2
    f32 = jnp.float32
    meet, fold, _ = fold_axes(me, col)
    loads = [
        pltpu.make_async_copy(a, b, load_sem.at[i])
        for i, (a, b) in enumerate(
            (
                (proj_hbm, proj),
                (sgate_hbm, sgate),
                (sup_hbm, sup),
                (gate_hbm, gate),
                (up_hbm, up),
                (sdown_hbm.at[col], sdown.at[0, 0]),
                (sdown_hbm.at[meet], sdown.at[0, 1]),
                (sdown_far_hbm, sdown.at[1]),
                (down_hbm.at[col], down.at[0, 0]),
                (down_hbm.at[meet], down.at[0, 1]),
                (down_far_hbm, down.at[1]),
            )
        )
    ]
    for load in loads:
        load.start()
    side = [flip(col, jnp.int32(j), 4) for j in range(4)]
    peer = lambda k: (flip(me, k, count), col)
    near_x, near_y = (me, side[1]), (me, side[2])
    greet([peer(jnp.int32(k)) for k in range(1, count)] + [near_x, near_y])

    def direct(buf, row, index):
        own = buf.at[(0,) + index]
        return (
            remote(own, buf.at[(1,) + index], gsend.at[row, 0], grecv.at[row, 0], near_x),
            remote(own, buf.at[(2,) + index], gsend.at[row, 1], grecv.at[row, 1], near_y),
        )

    def relays(buf, row, index):
        middle = buf.shape[-2] // 2
        top, low = pl.ds(0, middle), pl.ds(middle, middle)
        return (
            remote(
                buf.at[(1,) + index + (top,)], buf.at[(3,) + index + (top,)],
                gsend.at[row, 2], grecv.at[row, 2], near_y,
            ),
            remote(
                buf.at[(2,) + index + (low,)], buf.at[(3,) + index + (low,)],
                gsend.at[row, 3], grecv.at[row, 3], near_x,
            ),
        )

    def offer(buf, row, index=()):
        for copy in direct(buf, row, index):
            copy.start()

    def pass_on(buf, row, index=()):
        for first, second in zip(direct(buf, row, index), relays(buf, row, index)):
            first.wait_recv()
            second.start()

    def finish(buf, row, index=()):
        for copy in relays(buf, row, index):
            copy.wait_recv()

    def drain(buf, row, index=()):
        for copy in direct(buf, row, index) + relays(buf, row, index):
            copy.wait_send()

    def join(buf, row, index=()):
        own, other = buf.at[(0,) + index], buf.at[(1,) + index]
        return remote(own, other, fsend.at[row, 0], frecv.at[row, 0], (me, meet))

    def hand_over(buf, row, index=()):
        own, other = buf.at[(0,) + index], buf.at[(1,) + index]
        return remote(own, other, fsend.at[row, 1], frecv.at[row, 1], (me, fold))

    row_head, row_hidden, row_shared = count, count + 2, count

    head_copies = []
    for k in reversed(range(1, count)):
        there = peer(jnp.int32(k))
        head_copies.append(
            remote(heads_ref.at[there[0]], held.at[me], hsend.at[k], hrecv.at[k], there)
        )
        head_copies[-1].start()
    held[me] = heads_ref[me]

    near = routes_ref[...] ^ me
    lane = lax.broadcasted_iota(jnp.int32, (128, rows), 0)
    hits = [near[j : j + 1, :] == lane for j in range(2)]
    present = hits[0] | hits[1]
    before = (
        lax.broadcasted_iota(jnp.int32, (rows, rows), 0)
        < lax.broadcasted_iota(jnp.int32, (rows, rows), 1)
    )
    place = jnp.dot(
        present.astype(f32).astype(jnp.bfloat16),
        before.astype(f32).astype(jnp.bfloat16),
        preferred_element_type=f32,
    )
    place = jnp.where(present, place, -1.0)
    slot = lax.broadcasted_iota(jnp.int32, (capacity, rows), 0).astype(f32)
    for k in range(count):
        onehot[k] = (slot == place[k : k + 1, :]).astype(f32).astype(jnp.bfloat16)
    portion = jnp.where(hits[0], weight_ref[0:1, :], 0.0) + jnp.where(
        hits[1], weight_ref[1:2, :], 0.0
    )
    portions = jnp.transpose(portion)

    for copy in head_copies:
        copy.wait_recv()
    for pair in range(count // 2):
        first, second = held[2 * pair], held[2 * pair + 1]
        cut = slice(2 * pair * width, 2 * (pair + 1) * width)
        for h in range(2):
            part = slice(h * width, (h + 1) * width)
            head_buf[0, h, :, cut] = jnp.concatenate([first[:, part], second[:, part]], axis=1)
    for h in range(2):
        offer(head_buf, row_head + h, (h,))
    loads[0].wait()
    totals = [jnp.dot(head_buf[0, h], proj[col], preferred_element_type=f32) for h in range(2)]
    for h in range(2):
        pass_on(head_buf, row_head + h, (h,))
    for h in range(2):
        total = totals[h]
        for j in (1, 2):
            total = total + jnp.dot(head_buf[j, h], proj[side[j]], preferred_element_type=f32)
        finish(head_buf, row_head + h, (h,))
        total = total + jnp.dot(head_buf[3, h], proj[side[3]], preferred_element_type=f32)
        span = slice(h * half, (h + 1) * half)
        hidden_buf[0, h] = (stream_ref[span, :].astype(f32) + total).astype(jnp.bfloat16)
        offer(hidden_buf, row_hidden + h, (h,))

    def dispatch_far(k):
        return remote(outgoing.at[0, k], rows_in.at[0, k], zsend.at[k], zrecv.at[k], peer(k))

    def dispatch_near(k):
        return remote(outgoing.at[:, k], rows_in.at[:, k], zsend.at[k], zrecv.at[k], peer(k))

    def chosen(k, j):
        block = hidden_buf[j].reshape(rows, cols)
        return jnp.dot(onehot[k], block, preferred_element_type=f32).astype(jnp.bfloat16)

    for k in range(4, count):
        outgoing[0, k] = chosen(k, 0)
        dispatch_far(jnp.int32(k)).start()
    for h in range(2):
        pass_on(hidden_buf, row_hidden + h, (h,))

    def scaled(blocks):
        wide = [block.astype(f32) for block in blocks]
        squares = wide[0] * wide[0]
        for block in wide[1:]:
            squares = squares + block * block
        scale = lax.rsqrt(jnp.sum(squares, axis=1, keepdims=True) / (4 * cols) + epsilon)
        return [
            (block * scale * gain_ref[side[j]]).astype(jnp.bfloat16)
            for j, block in enumerate(wide)
        ]

    def gated_pair(blocks, first, second):
        gated, lifted = [
            sum(jnp.dot(block, w[side[j]], preferred_element_type=f32) for j, block in enumerate(blocks))
            for w in (first, second)
        ]
        return (jax.nn.silu(gated) * lifted).astype(jnp.bfloat16)

    for h in range(2):
        finish(hidden_buf, row_hidden + h, (h,))
    for j in range(4):
        outgoing[j, 1] = chosen(1, j)
    dispatch_near(jnp.int32(1)).start()
    for k in (2, 3):
        for j in range(4):
            outgoing[j, k] = chosen(k, j)
        dispatch_near(jnp.int32(k)).start()
    for j in range(4):
        rows_in[j, 0] = chosen(0, j)
    for h in range(2):
        span = slice(h * half, (h + 1) * half)
        for j, block in enumerate(scaled([hidden_buf[j, h] for j in range(4)])):
            normed[j, span, :] = block
    for load in loads[1:]:
        load.wait()
    dispatch_far(jnp.int32(4)).wait_recv()
    offer(rows_in, 4, (4,))

    def give_back(k):
        return remote(made.at[k], back.at[k], rsend.at[k], rrecv.at[k], peer(k))

    def turn(p):
        later = jnp.where(p < count - 2, p + 2, p - count + 4)
        return jnp.where(p < 2, p, later)

    @pl.loop(0, count + 2)
    def _(i):
        @pl.when((i >= 2) & (i < count - 2))
        def _():
            finish(rows_in, i + 2, (i + 2,))

        @pl.when((i == 1) | ((i >= count - 2) & (i < count)))
        def _():
            dispatch_near(turn(i)).wait_recv()

        @pl.when(i < count)
        def _():
            k = turn(i)
            acts[0, k] = gated_pair(scaled([rows_in[j, k] for j in range(4)]), gate, up)
            join(acts, k, (k,)).start()

        @pl.when(i == 0)
        def _():
            shared_buf[0] = gated_pair([normed[j] for j in range(4)], sgate, sup)
            join(shared_buf, row_shared).start()

        @pl.when(i < count - 5)
        def _():
            dispatch_far(i + 5).wait_recv()
            offer(rows_in, i + 5, (i + 5,))

        @pl.when(i < count - 4)
        def _():
            pass_on(rows_in, i + 4, (i + 4,))

        @pl.when((i >= 1) & (i < count + 1))
        def _():
            k = turn(i - 1)
            join(acts, k, (k,)).wait_recv()
            own, other = [
                jnp.dot(acts[0, k], down[c, 0], preferred_element_type=f32)
                + jnp.dot(acts[1, k], down[c, 1], preferred_element_type=f32)
                for c in range(2)
            ]
            parts[0, k] = other.astype(jnp.bfloat16)
            hand_over(parts, k, (k,)).start()
            kept[k] = own

        @pl.when(i == 1)
        def _():
            join(shared_buf, row_shared).wait_recv()
            own, other = [
                jnp.dot(shared_buf[0], sdown[c, 0], preferred_element_type=f32)
                + jnp.dot(shared_buf[1], sdown[c, 1], preferred_element_type=f32)
                for c in range(2)
            ]
            shared_part[0] = other.astype(jnp.bfloat16)
            hand_over(shared_part, row_shared).start()
            shared_cols[...] = own

        @pl.when(i >= 2)
        def _():
            k = turn(i - 2)
            hand_over(parts, k, (k,)).wait_recv()
            made[k] = (kept[k] + parts[1, k].astype(f32)).astype(jnp.bfloat16)

            @pl.when(k > 0)
            def _():
                give_back(k).start()

    hand_over(shared_part, row_shared).wait_recv()
    shared_cols[...] = shared_cols[...] + shared_part[1].astype(f32)
    back[0] = made[0]
    for p in range(count):
        k = p if p < 2 else (p + 2 if p < count - 2 else p - count + 4)
        if k > 0:
            give_back(jnp.int32(k)).wait_recv()
        picked = lax.dot_general(
            onehot[k], back[k], (((0,), (0,)), ((), ())), preferred_element_type=f32
        )
        shared_cols[...] = shared_cols[...] + portions[:, k : k + 1] * picked
    for h in range(2):
        span = slice(h * half, (h + 1) * half)
        out_ref[span, :] = (hidden_buf[0, h].astype(f32) + shared_cols[span, :]).astype(
            jnp.bfloat16
        )

    for copy in head_copies:
        copy.wait_send()
    for h in range(2):
        drain(head_buf, row_head + h, (h,))
        drain(hidden_buf, row_hidden + h, (h,))
    join(shared_buf, row_shared).wait_send()
    hand_over(shared_part, row_shared).wait_send()

    @pl.loop(4, count)
    def _(k):
        drain(rows_in, k, (k,))
        dispatch_far(k).wait_send()

    @pl.loop(1, 4)
    def _(k):
        dispatch_near(k).wait_send()

    @pl.loop(0, count)
    def _(k):
        join(acts, k, (k,)).wait_send()
        hand_over(parts, k, (k,)).wait_send()

        @pl.when(k > 0)
        def _():
            give_back(k).wait_send()


def head_per_device(
    query_pairs,
    key_pairs,
    value_rows,
    doc_ids,
    contrast_lambda,
    head_gain,
    stream,
    out_proj,
    norm_gain,
    routes,
    route_weights,
    expert_gate,
    expert_up,
    expert_down,
    shared_gate,
    shared_up,
    shared_down,
):
    rows, cols = stream.shape
    count, sides = lax.axis_size("sp"), lax.axis_size("tp")
    width = value_rows.shape[1] // count
    capacity = 2 * rows * routes.shape[1] // count
    bf16, f32 = jnp.bfloat16, jnp.float32
    dma = pltpu.SemaphoreType.DMA
    split = lambda weight: weight.reshape(sides, weight.shape[-2] // sides, weight.shape[-1])
    down, sdown = split(expert_down[0]), split(shared_down)
    qkv, docs, down_far, sdown_far = pl.pallas_call(
        functools.partial(spread_kernel, count, width),
        out_shape=(
            jax.ShapeDtypeStruct((count, rows + rows // 2, 2 * width), bf16),
            jax.ShapeDtypeStruct((count, 1, rows), jnp.int32),
            jax.ShapeDtypeStruct((2, cols, cols), bf16),
            jax.ShapeDtypeStruct((2, cols, cols), bf16),
        ),
        in_specs=[VMEM] * 4 + [ANY] * 2,
        out_specs=(VMEM, VMEM, ANY, ANY),
        scratch_shapes=[
            pltpu.VMEM((count, rows + rows // 2, 2 * width), bf16),
            dma((count,)),
            dma((count,)),
            dma((count,)),
            dma((count,)),
            dma((2, 2)),
            dma((2, 2)),
        ],
        compiler_params=pltpu.CompilerParams(collective_id=0, has_side_effects=True),
        name="spread_heads",
    )(query_pairs, key_pairs, value_rows, doc_ids.reshape(1, rows), down, sdown)
    heads = pl.pallas_call(
        functools.partial(attend_kernel, (width // 2) ** (-0.5)),
        out_shape=jax.ShapeDtypeStruct((count, rows // 2, 2 * width), bf16),
        in_specs=[SMEM, VMEM, VMEM, VMEM],
        out_specs=VMEM,
        scratch_shapes=[pltpu.VMEM((count, 2 * width, rows // 2), bf16)],
        name="attend",
    )(
        contrast_lambda,
        qkv,
        docs,
        head_gain.reshape(1, width),
    )
    weight_shape = (sides, cols, cols)
    slots = (count, capacity, cols)
    return pl.pallas_call(
        functools.partial(layer_kernel, count, capacity),
        out_shape=jax.ShapeDtypeStruct((rows, cols), bf16),
        in_specs=[VMEM] * 5 + [ANY] * 9,
        out_specs=VMEM,
        scratch_shapes=[pltpu.VMEM(weight_shape, bf16)] * 5
        + [pltpu.VMEM((2, 2, cols, cols), bf16)] * 2
        + [
            pltpu.VMEM((count, rows // 2, 2 * width), bf16),
            pltpu.VMEM((sides, 2, rows // 2, cols), bf16),
            pltpu.VMEM((sides, 2, rows // 2, cols), bf16),
            pltpu.VMEM((sides, rows, cols), bf16),
            pltpu.VMEM((2, rows, cols), bf16),
            pltpu.VMEM((2, rows, cols), bf16),
            pltpu.VMEM((count, capacity, rows), bf16),
            pltpu.VMEM((sides,) + slots, bf16),
            pltpu.VMEM((sides,) + slots, bf16),
            pltpu.VMEM((2,) + slots, bf16),
            pltpu.VMEM((2,) + slots, bf16),
            pltpu.VMEM(slots, f32),
            pltpu.VMEM(slots, bf16),
            pltpu.VMEM(slots, bf16),
            pltpu.VMEM((rows, cols), f32),
            dma((11,)),
            dma((count,)),
            dma((count,)),
            dma((count + 4, 4)),
            dma((count + 4, 4)),
            dma((count + 1, 2)),
            dma((count + 1, 2)),
            dma((count,)),
            dma((count,)),
            dma((count,)),
            dma((count,)),
        ],
        compiler_params=pltpu.CompilerParams(
            collective_id=1, has_side_effects=True, vmem_limit_bytes=60 * 2**20
        ),
        name="layer",
    )(
        heads,
        stream,
        norm_gain.reshape(sides, 1, cols),
        routes.T,
        route_weights.T,
        split(out_proj),
        split(shared_gate),
        split(shared_up),
        split(expert_gate[0]),
        split(expert_up[0]),
        sdown,
        down,
        sdown_far,
        down_far,
    )


def choose(*args):
    query_pairs, value_rows, heads, stream = args[0], args[2], args[4].shape[0], args[6]
    count, sides = lax.axis_size("sp"), lax.axis_size("tp")
    width = value_rows.shape[1] // heads
    rows, cols = stream.shape
    hidden = {args[i].shape[-1] for i in (7, 11, 12, 13, 14, 15, 16)}
    fits = (
        heads == count
        and count & (count - 1) == 0
        and 8 <= count <= 128
        and sides == 4
        and 2 * width == 128
        and query_pairs.shape[1] == value_rows.shape[1] == cols
        and hidden == {cols}
        and all(args[i].shape[-2] == sides * cols for i in (7, 11, 12, 13, 14, 15, 16))
        and rows % 256 == 0
        and (2 * rows * args[9].shape[1]) % (128 * count) == 0
        and args[9].shape[1] == 2
    )
    return (head_per_device if fits else shards)(*args)


def solution(mesh):
    return jax.shard_map(
        choose,
        mesh=mesh,
        in_specs=(
            P("sp", "tp"),
            P("sp", "tp"),
            P("sp", "tp"),
            P("sp"),
            P("tp"),
            P(),
            P("sp", "tp"),
            P(None, "tp"),
            P(),
            P("sp", None),
            P("sp", None),
            P("sp", None, "tp"),
            P("sp", None, "tp"),
            P("sp", None, "tp"),
            P(None, "tp"),
            P(None, "tp"),
            P(None, "tp"),
        ),
        out_specs=P("sp", "tp"),
        check_vma=False,
    )
```

```python
import functools
import math

import jax
import jax.numpy as jnp
from jax import lax
from jax.experimental import pallas as pl
from jax.experimental.pallas import tpu as pltpu
from jax.sharding import PartitionSpec as P

epsilon = 1e-06
floor_score = -1e30


def add_columns(weight_rows, part_block):
    return jnp.dot(part_block, weight_rows, preferred_element_type=jnp.float32)


def shards(
    query_pairs,
    key_pairs,
    value_rows,
    doc_ids,
    contrast_lambda,
    head_gain,
    stream,
    out_proj,
    norm_gain,
    routes,
    route_weights,
    expert_gate,
    expert_up,
    expert_down,
    shared_gate,
    shared_up,
    shared_down,
):
    row_count = query_pairs.shape[0]
    local_heads = contrast_lambda.shape[0]
    key_width = query_pairs.shape[1] // (2 * local_heads)
    value_width = value_rows.shape[1] // local_heads
    scaling = key_width ** (-0.5)
    first_row = lax.axis_index("sp") * row_count
    query_pos = first_row + jnp.arange(row_count, dtype=jnp.int32)
    last_query = first_row + row_count - 1
    first_doc = doc_ids[0]
    query_split = query_pairs.reshape(row_count, local_heads, 2, key_width)

    def absorb_block(running, key_block, value_block, doc_block, key_start):
        best, denom, numer = running
        span_len = key_block.shape[0]
        key_pos = key_start + jnp.arange(span_len, dtype=jnp.int32)
        allowed = (key_pos[None, :] <= query_pos[:, None]) & (
            doc_block[None, :] == doc_ids[:, None]
        )
        scores = (
            jnp.einsum(
                "qhmd,khmd->hmqk",
                query_split,
                key_block.reshape(span_len, local_heads, 2, key_width),
                preferred_element_type=jnp.float32,
            )
            * scaling
        )
        scores = jnp.where(allowed, scores, floor_score)
        new_best = jnp.maximum(best, jnp.max(scores, axis=-1))
        weights = jnp.where(allowed, jnp.exp(scores - new_best[..., None]), 0.0)
        fade = jnp.exp(best - new_best)
        denom = denom * fade + jnp.sum(weights, axis=-1)
        numer = numer * fade[..., None] + jnp.einsum(
            "hmqk,khv->hmqv",
            weights.astype(jnp.bfloat16),
            value_block.reshape(span_len, local_heads, value_width),
            preferred_element_type=jnp.float32,
        )
        return (new_best, denom, numer)

    start_best = jnp.full((local_heads, 2, row_count), floor_score, jnp.float32)
    start_denom = jnp.zeros((local_heads, 2, row_count), jnp.float32)
    start_numer = jnp.zeros((local_heads, 2, row_count, value_width), jnp.float32)
    key_piece = lax.all_gather(key_pairs, "sp", axis=0, tiled=True)
    value_piece = lax.all_gather(value_rows, "sp", axis=0, tiled=True)
    doc_piece = lax.all_gather(doc_ids, "sp", axis=0, tiled=True)
    length = key_piece.shape[0]
    span_len = row_count * max(1, 512 // row_count)

    def one_span(span_index, carried):
        offset = span_index * span_len
        key_block = lax.dynamic_slice_in_dim(key_piece, offset, span_len, 0)
        value_block = lax.dynamic_slice_in_dim(value_piece, offset, span_len, 0)
        doc_block = lax.dynamic_slice_in_dim(doc_piece, offset, span_len, 0)
        needed = (offset <= last_query) & (doc_block[span_len - 1] >= first_doc)
        return lax.cond(
            needed,
            lambda held: absorb_block(held, key_block, value_block, doc_block, offset),
            lambda held: held,
            carried,
        )

    best, denom, numer = lax.fori_loop(
        0, length // span_len, one_span, (start_best, start_denom, start_numer)
    )
    heard = numer / denom[..., None]
    contrast = heard[:, 0] - contrast_lambda[:, None, None] * heard[:, 1]
    contrast = (
        contrast
        * lax.rsqrt(jnp.mean(contrast * contrast, axis=-1, keepdims=True) + epsilon)
        * head_gain
    )
    head_out = (
        jnp.transpose(contrast, (1, 0, 2))
        .reshape(row_count, local_heads * value_width)
        .astype(jnp.bfloat16)
    )
    projected = add_columns(out_proj, lax.all_gather(head_out, "tp", axis=1, tiled=True))
    hidden_cols = (stream.astype(jnp.float32) + projected).astype(jnp.bfloat16)
    hidden_rows = lax.all_gather(hidden_cols, "tp", axis=1, tiled=True)
    widened = hidden_rows.astype(jnp.float32)
    normed = (
        widened
        * lax.rsqrt(jnp.mean(widened * widened, axis=-1, keepdims=True) + epsilon)
        * norm_gain
    ).astype(jnp.bfloat16)
    shared_act = (
        jax.nn.silu(jnp.dot(normed, shared_gate, preferred_element_type=jnp.float32))
        * jnp.dot(normed, shared_up, preferred_element_type=jnp.float32)
    ).astype(jnp.bfloat16)
    shared_cols = add_columns(shared_down, lax.all_gather(shared_act, "tp", axis=1, tiled=True))
    expert_count = lax.axis_size("sp")
    route_count = routes.shape[1]
    capacity = 2 * row_count * route_count // expert_count
    flat_routes = routes.reshape(-1)
    hits = (flat_routes[:, None] == jnp.arange(expert_count, dtype=jnp.int32)[None, :]).astype(
        jnp.int32
    )
    position = jnp.sum(jnp.cumsum(hits, axis=0) * hits, axis=1) - 1
    target = flat_routes * capacity + position
    sources = jnp.arange(flat_routes.shape[0], dtype=jnp.int32) // route_count
    owner = jnp.zeros((expert_count * capacity,), jnp.int32).at[target].set(sources)
    outgoing = normed[owner].reshape(expert_count, capacity, normed.shape[1])
    gate_cols = expert_gate[0]
    up_cols = expert_up[0]
    down_cols = expert_down[0]
    slice_width = outgoing.shape[2] // lax.axis_size("tp")
    own_slice = lax.dynamic_slice_in_dim(
        outgoing, lax.axis_index("tp") * slice_width, slice_width, 2
    )
    arrived = lax.all_to_all(own_slice, "sp", split_axis=0, concat_axis=0, tiled=True)
    apply_arrived = lax.all_gather(arrived, "tp", axis=2, tiled=True)
    gated = jnp.einsum("snd,df->snf", apply_arrived, gate_cols, preferred_element_type=jnp.float32)
    lifted = jnp.einsum("snd,df->snf", apply_arrived, up_cols, preferred_element_type=jnp.float32)
    expert_act = (jax.nn.silu(gated) * lifted).astype(jnp.bfloat16)
    expert_out = add_columns(
        down_cols, lax.all_gather(expert_act, "tp", axis=2, tiled=True)
    ).astype(jnp.bfloat16)
    returned = lax.all_to_all(expert_out, "sp", split_axis=0, concat_axis=0, tiled=True)
    flat_back = returned.reshape(expert_count * capacity, returned.shape[2])
    picked = (
        flat_back[target].reshape(row_count, route_count, returned.shape[2]).astype(jnp.float32)
    )
    routed = jnp.sum(picked * route_weights[:, :, None], axis=1)
    return (hidden_cols.astype(jnp.float32) + shared_cols + routed).astype(jnp.bfloat16)


MESH_ID = pl.DeviceIdType.MESH
VMEM = pl.BlockSpec(memory_space=pltpu.VMEM)
ANY = pl.BlockSpec(memory_space=pl.ANY)
SMEM = pl.BlockSpec(memory_space=pltpu.SMEM)


def flip(index, mask, size):
    out, bit = 0, 1
    while bit < size:
        out = out + bit * lax.rem(lax.div(index, bit) + lax.div(mask, bit), 2)
        bit *= 2
    return out


def remote(src, dst, send, recv, device):
    return pltpu.make_async_remote_copy(
        src_ref=src,
        dst_ref=dst,
        send_sem=send,
        recv_sem=recv,
        device_id=device,
        device_id_type=MESH_ID,
    )


def greet(devices):
    barrier = pltpu.get_barrier_semaphore()
    for device in devices:
        pl.semaphore_signal(barrier, inc=1, device_id=device, device_id_type=MESH_ID)
    pl.semaphore_wait(barrier, len(devices))


def fold_axes(me, col):
    core = lax.rem(me, 2)
    return flip(col, 2 - core, 4), flip(col, 1 + core, 4), flip(col, jnp.int32(3), 4)


def layer_kernel(
    count,
    capacity,
    scaling,
    lam_ref,
    q_ref,
    k_ref,
    v_ref,
    doc_ref,
    head_gain_ref,
    stream_ref,
    gain_ref,
    routes_ref,
    weight_ref,
    proj_hbm,
    sgate_hbm,
    sup_hbm,
    gate_hbm,
    up_hbm,
    sdown_hbm,
    down_hbm,
    out_ref,
    pack,
    qkv,
    docs,
    doc_cols,
    queries,
    turned,
    best_ref,
    denom_ref,
    numer_ref,
    head_out,
    portions,
    proj,
    sgate,
    sup,
    gate,
    up,
    sdown,
    down,
    held,
    head_buf,
    hidden_buf,
    normed,
    shared_buf,
    shared_part,
    onehot,
    outgoing,
    rows_in,
    acts,
    parts,
    kept,
    made,
    back,
    shared_cols,
    load_sem,
    xsend,
    xrecv,
    wsend,
    wrecv,
    hsend,
    hrecv,
    gsend,
    grecv,
    fsend,
    frecv,
    zsend,
    zrecv,
    rsend,
    rrecv,
):
    me, col = lax.axis_index("sp"), lax.axis_index("tp")
    rows, cols = stream_ref.shape
    half = rows // 2
    width = head_gain_ref.shape[1]
    key_width = width // 2
    f32 = jnp.float32
    meet, fold, across = fold_axes(me, col)
    loads = [
        pltpu.make_async_copy(a, b, load_sem.at[i])
        for i, (a, b) in enumerate(
            (
                (proj_hbm, proj),
                (sgate_hbm, sgate),
                (sup_hbm, sup),
                (gate_hbm, gate),
                (up_hbm, up),
                (sdown_hbm.at[col], sdown.at[0, 0]),
                (sdown_hbm.at[meet], sdown.at[0, 1]),
                (down_hbm.at[col], down.at[0, 0]),
                (down_hbm.at[meet], down.at[0, 1]),
            )
        )
    ]
    for load in loads:
        load.start()
    side = [flip(col, jnp.int32(j), 4) for j in range(4)]
    peer = lambda k: (flip(me, k, count), col)
    near_x, near_y = (me, side[1]), (me, side[2])
    for h in range(count):
        cut = slice(h * width, (h + 1) * width)
        pack[h, :rows, :] = jnp.concatenate([q_ref[:, cut], k_ref[:, cut]], axis=1)
        pack[h, rows:, :] = jnp.concatenate([v_ref[:half, cut], v_ref[half:, cut]], axis=1)
    greet([peer(jnp.int32(k)) for k in range(1, count)] + [near_x, near_y])

    def direct(buf, row, index):
        own = buf.at[(0,) + index]
        return (
            remote(own, buf.at[(1,) + index], gsend.at[row, 0], grecv.at[row, 0], near_x),
            remote(own, buf.at[(2,) + index], gsend.at[row, 1], grecv.at[row, 1], near_y),
        )

    def relays(buf, row, index):
        middle = buf.shape[-2] // 2
        top, low = pl.ds(0, middle), pl.ds(middle, middle)
        return (
            remote(
                buf.at[(1,) + index + (top,)], buf.at[(3,) + index + (top,)],
                gsend.at[row, 2], grecv.at[row, 2], near_y,
            ),
            remote(
                buf.at[(2,) + index + (low,)], buf.at[(3,) + index + (low,)],
                gsend.at[row, 3], grecv.at[row, 3], near_x,
            ),
        )

    def offer(buf, row, index=()):
        for copy in direct(buf, row, index):
            copy.start()

    def pass_on(buf, row, index=()):
        for first, second in zip(direct(buf, row, index), relays(buf, row, index)):
            first.wait_recv()
            second.start()

    def finish(buf, row, index=()):
        for copy in relays(buf, row, index):
            copy.wait_recv()

    def drain(buf, row, index=()):
        for copy in direct(buf, row, index) + relays(buf, row, index):
            copy.wait_send()

    def join(buf, row, index=()):
        own, other = buf.at[(0,) + index], buf.at[(1,) + index]
        return remote(own, other, fsend.at[row, 0], frecv.at[row, 0], (me, meet))

    def hand_over(buf, row, index=()):
        own, other = buf.at[(0,) + index], buf.at[(1,) + index]
        return remote(own, other, fsend.at[row, 1], frecv.at[row, 1], (me, fold))

    row_head, row_hidden, row_shared = count, count + 2, count

    def exchange(k):
        there = peer(k)
        return (
            remote(doc_ref, docs.at[me], xsend.at[0, k], xrecv.at[0, k], there),
            remote(pack.at[there[0]], qkv.at[me], xsend.at[1, k], xrecv.at[1, k], there),
        )

    def head_copy(k):
        there = peer(k)
        return remote(head_out.at[there[0]], held.at[me], hsend.at[k], hrecv.at[k], there)

    swaps = [
        remote(src.at[quarter], dst.at[1, i], wsend.at[j, i], wrecv.at[j, i], (me, fold))
        for j, (src, dst) in enumerate(((down_hbm, down), (sdown_hbm, sdown)))
        for i, quarter in enumerate((fold, across))
    ]
    for k in range(1, count):
        for copy in exchange(jnp.int32(k)):
            copy.start()
    for swap in swaps:
        swap.start()
    qkv[me] = pack[me]
    docs[me] = doc_ref[...]
    best_ref[...] = jnp.full(best_ref.shape, floor_score, f32)
    denom_ref[...] = jnp.zeros(denom_ref.shape, f32)
    numer_ref[...] = jnp.zeros(numer_ref.shape, f32)

    near = routes_ref[...] ^ me
    lane = lax.broadcasted_iota(jnp.int32, (128, rows), 0)
    hits = [near[j : j + 1, :] == lane for j in range(2)]
    present = hits[0] | hits[1]
    before = (
        lax.broadcasted_iota(jnp.int32, (rows, rows), 0)
        < lax.broadcasted_iota(jnp.int32, (rows, rows), 1)
    )
    place = jnp.dot(
        present.astype(f32).astype(jnp.bfloat16),
        before.astype(f32).astype(jnp.bfloat16),
        preferred_element_type=f32,
    )
    place = jnp.where(present, place, -1.0)
    slot = lax.broadcasted_iota(jnp.int32, (capacity, rows), 0).astype(f32)
    for k in range(count):
        onehot[k] = (slot == place[k : k + 1, :]).astype(f32).astype(jnp.bfloat16)
    portion = jnp.where(hits[0], weight_ref[0:1, :], 0.0) + jnp.where(
        hits[1], weight_ref[1:2, :], 0.0
    )
    portions[...] = jnp.transpose(portion)

    weight = lam_ref[me]
    gains = jnp.concatenate([head_gain_ref[...], head_gain_ref[...]], axis=1)
    factor = scaling * math.log2(math.e)
    lanes = lax.broadcasted_iota(jnp.int32, (rows, 2 * width), 1)

    @pl.loop(0, count)
    def _(i):
        j = flip(me, i, count)

        @pl.when(i > 0)
        def _():
            for copy in exchange(i):
                copy.wait_recv()

        values = jnp.transpose(qkv[j, rows:, :].astype(f32)).astype(jnp.bfloat16)
        turned[j] = jnp.concatenate([values[:width], values[width:]], axis=1)
        moved = pltpu.roll(qkv[j, :rows, :].astype(f32), width, 1)
        for m in range(2):
            begin = width + m * key_width
            inside = (lanes >= begin) & (lanes < begin + key_width)
            queries[j, m] = jnp.where(inside, moved, 0.0).astype(jnp.bfloat16)
        doc_cols[j] = jnp.transpose(jnp.broadcast_to(docs[j].astype(f32), (8, rows)))

        def pair_of_tiles(step, carried):
            ahead = lax.broadcasted_iota(jnp.int32, (rows, rows), 0) - lax.broadcasted_iota(
                jnp.int32, (rows, rows), 1
            )
            tiles = []
            for part in range(2):
                second = 2 * step + part
                other = flip(me, jnp.minimum(second, i), count)
                q, k = jnp.maximum(j, other), jnp.minimum(j, other)
                limit = jnp.where(second <= i, (q - k) * rows, -rows)
                allowed = (ahead <= limit) & (doc_cols[k][:, 0:1] == docs[q].astype(f32))
                tiles.append((q, k, allowed))
            scores = [
                [
                    jnp.where(
                        allowed,
                        lax.dot_general(
                            qkv[k, :rows, :], queries[q, m], (((1,), (1,)), ((), ())),
                            preferred_element_type=f32,
                        )
                        * factor,
                        floor_score,
                    )
                    for m in range(2)
                ]
                for q, k, allowed in tiles
            ]
            for part, (q, k, _) in enumerate(tiles):
                for m in range(2):
                    row = pl.ds(2 * part + m, 1)
                    tile = scores[part][m]
                    best = best_ref[q, row, :]
                    new_best = jnp.maximum(best, jnp.max(tile, axis=0, keepdims=True))
                    fade = jnp.exp2(best - new_best)
                    weights = jnp.exp2(tile - new_best)
                    best_ref[q, row, :] = new_best
                    denom_ref[q, row, :] = denom_ref[q, row, :] * fade + jnp.sum(
                        weights, axis=0, keepdims=True
                    )
                    numer_ref[q, 2 * part + m] = numer_ref[q, 2 * part + m] * fade + jnp.dot(
                        turned[k], weights.astype(jnp.bfloat16), preferred_element_type=f32
                    )
            return carried

        lax.fori_loop(0, lax.div(i, 2) + 1, pair_of_tiles, 0)

    @pl.loop(0, count)
    def _(i):
        k = count - 1 - i
        b = flip(me, k, count)
        heard = []
        for m in range(2):
            bests = [best_ref[b, pl.ds(2 * part + m, 1), :] for part in range(2)]
            top = jnp.maximum(*bests)
            fades = [jnp.exp2(best - top) for best in bests]
            denom, numer = [
                first * fades[0] + second * fades[1]
                for first, second in (
                    [denom_ref[b, pl.ds(2 * part + m, 1), :] for part in range(2)],
                    [numer_ref[b, 2 * part + m] for part in range(2)],
                )
            ]
            heard.append(numer / denom)
        contrast = heard[0] - weight * heard[1]
        contrast = contrast * lax.rsqrt(
            jnp.mean(contrast * contrast, axis=0, keepdims=True) + epsilon
        )
        stacked = jnp.concatenate([contrast[:, :half], contrast[:, half:]], axis=0)
        head_out[b] = (jnp.transpose(stacked) * gains).astype(jnp.bfloat16)

        @pl.when(k > 0)
        def _():
            head_copy(k).start()

    held[me] = head_out[me]

    @pl.loop(1, count)
    def _(k):
        head_copy(k).wait_recv()

    for pair in range(count // 2):
        first, second = held[2 * pair], held[2 * pair + 1]
        cut = slice(2 * pair * width, 2 * (pair + 1) * width)
        for h in range(2):
            part = slice(h * width, (h + 1) * width)
            head_buf[0, h, :, cut] = jnp.concatenate([first[:, part], second[:, part]], axis=1)
    for h in range(2):
        offer(head_buf, row_head + h, (h,))
    loads[0].wait()
    totals = [jnp.dot(head_buf[0, h], proj[col], preferred_element_type=f32) for h in range(2)]
    for h in range(2):
        pass_on(head_buf, row_head + h, (h,))
    for h in range(2):
        total = totals[h]
        for j in (1, 2):
            total = total + jnp.dot(head_buf[j, h], proj[side[j]], preferred_element_type=f32)
        finish(head_buf, row_head + h, (h,))
        total = total + jnp.dot(head_buf[3, h], proj[side[3]], preferred_element_type=f32)
        span = slice(h * half, (h + 1) * half)
        hidden_buf[0, h] = (stream_ref[span, :].astype(f32) + total).astype(jnp.bfloat16)
        offer(hidden_buf, row_hidden + h, (h,))

    def dispatch_far(k):
        return remote(outgoing.at[0, k], rows_in.at[0, k], zsend.at[k], zrecv.at[k], peer(k))

    def dispatch_near(k):
        return remote(outgoing.at[:, k], rows_in.at[:, k], zsend.at[k], zrecv.at[k], peer(k))

    def chosen(k, j):
        block = hidden_buf[j].reshape(rows, cols)
        return jnp.dot(onehot[k], block, preferred_element_type=f32).astype(jnp.bfloat16)

    for k in range(4, count):
        outgoing[0, k] = chosen(k, 0)
        dispatch_far(jnp.int32(k)).start()
    for h in range(2):
        pass_on(hidden_buf, row_hidden + h, (h,))

    def scaled(blocks):
        wide = [block.astype(f32) for block in blocks]
        squares = wide[0] * wide[0]
        for block in wide[1:]:
            squares = squares + block * block
        scale = lax.rsqrt(jnp.sum(squares, axis=1, keepdims=True) / (4 * cols) + epsilon)
        return [
            (block * scale * gain_ref[side[j]]).astype(jnp.bfloat16)
            for j, block in enumerate(wide)
        ]

    def gated_pair(blocks, first, second):
        gated, lifted = [
            sum(jnp.dot(block, w[side[j]], preferred_element_type=f32) for j, block in enumerate(blocks))
            for w in (first, second)
        ]
        return (jax.nn.silu(gated) * lifted).astype(jnp.bfloat16)

    for h in range(2):
        finish(hidden_buf, row_hidden + h, (h,))
    for j in range(4):
        outgoing[j, 1] = chosen(1, j)
    dispatch_near(jnp.int32(1)).start()
    for k in (2, 3):
        for j in range(4):
            outgoing[j, k] = chosen(k, j)
        dispatch_near(jnp.int32(k)).start()
    for j in range(4):
        rows_in[j, 0] = chosen(0, j)
    for h in range(2):
        span = slice(h * half, (h + 1) * half)
        for j, block in enumerate(scaled([hidden_buf[j, h] for j in range(4)])):
            normed[j, span, :] = block
    for load in loads[1:]:
        load.wait()
    for swap in swaps:
        swap.wait_recv()
    dispatch_far(jnp.int32(4)).wait_recv()
    offer(rows_in, 4, (4,))

    def give_back(k):
        return remote(made.at[k], back.at[k], rsend.at[k], rrecv.at[k], peer(k))

    def turn(p):
        later = jnp.where(p < count - 2, p + 2, p - count + 4)
        return jnp.where(p < 2, p, later)

    @pl.loop(0, count + 2)
    def _(i):
        @pl.when((i >= 2) & (i < count - 2))
        def _():
            finish(rows_in, i + 2, (i + 2,))

        @pl.when((i == 1) | ((i >= count - 2) & (i < count)))
        def _():
            dispatch_near(turn(i)).wait_recv()

        @pl.when(i < count)
        def _():
            k = turn(i)
            acts[0, k] = gated_pair(scaled([rows_in[j, k] for j in range(4)]), gate, up)
            join(acts, k, (k,)).start()

        @pl.when(i == 0)
        def _():
            shared_buf[0] = gated_pair([normed[j] for j in range(4)], sgate, sup)
            join(shared_buf, row_shared).start()

        @pl.when(i < count - 5)
        def _():
            dispatch_far(i + 5).wait_recv()
            offer(rows_in, i + 5, (i + 5,))

        @pl.when(i < count - 4)
        def _():
            pass_on(rows_in, i + 4, (i + 4,))

        @pl.when((i >= 1) & (i < count + 1))
        def _():
            k = turn(i - 1)
            join(acts, k, (k,)).wait_recv()
            own, other = [
                jnp.dot(acts[0, k], down[c, 0], preferred_element_type=f32)
                + jnp.dot(acts[1, k], down[c, 1], preferred_element_type=f32)
                for c in range(2)
            ]
            parts[0, k] = other.astype(jnp.bfloat16)
            hand_over(parts, k, (k,)).start()
            kept[k] = own

        @pl.when(i == 1)
        def _():
            join(shared_buf, row_shared).wait_recv()
            own, other = [
                jnp.dot(shared_buf[0], sdown[c, 0], preferred_element_type=f32)
                + jnp.dot(shared_buf[1], sdown[c, 1], preferred_element_type=f32)
                for c in range(2)
            ]
            shared_part[0] = other.astype(jnp.bfloat16)
            hand_over(shared_part, row_shared).start()
            shared_cols[...] = own

        @pl.when(i >= 2)
        def _():
            k = turn(i - 2)
            hand_over(parts, k, (k,)).wait_recv()
            made[k] = (kept[k] + parts[1, k].astype(f32)).astype(jnp.bfloat16)

            @pl.when(k > 0)
            def _():
                give_back(k).start()

    hand_over(shared_part, row_shared).wait_recv()
    shared_cols[...] = shared_cols[...] + shared_part[1].astype(f32)
    back[0] = made[0]
    for p in range(count):
        k = p if p < 2 else (p + 2 if p < count - 2 else p - count + 4)
        if k > 0:
            give_back(jnp.int32(k)).wait_recv()
        picked = lax.dot_general(
            onehot[k], back[k], (((0,), (0,)), ((), ())), preferred_element_type=f32
        )
        shared_cols[...] = shared_cols[...] + portions[:, k : k + 1] * picked
    for h in range(2):
        span = slice(h * half, (h + 1) * half)
        out_ref[span, :] = (hidden_buf[0, h].astype(f32) + shared_cols[span, :]).astype(
            jnp.bfloat16
        )

    for swap in swaps:
        swap.wait_send()
    for h in range(2):
        drain(head_buf, row_head + h, (h,))
        drain(hidden_buf, row_hidden + h, (h,))
    join(shared_buf, row_shared).wait_send()
    hand_over(shared_part, row_shared).wait_send()

    @pl.loop(4, count)
    def _(k):
        drain(rows_in, k, (k,))
        dispatch_far(k).wait_send()

    @pl.loop(1, 4)
    def _(k):
        dispatch_near(k).wait_send()

    @pl.loop(1, count)
    def _(k):
        head_copy(k).wait_send()
        for copy in exchange(k):
            copy.wait_send()

    @pl.loop(0, count)
    def _(k):
        join(acts, k, (k,)).wait_send()
        hand_over(parts, k, (k,)).wait_send()

        @pl.when(k > 0)
        def _():
            give_back(k).wait_send()


def head_per_device(
    query_pairs,
    key_pairs,
    value_rows,
    doc_ids,
    contrast_lambda,
    head_gain,
    stream,
    out_proj,
    norm_gain,
    routes,
    route_weights,
    expert_gate,
    expert_up,
    expert_down,
    shared_gate,
    shared_up,
    shared_down,
):
    rows, cols = stream.shape
    count, sides = lax.axis_size("sp"), lax.axis_size("tp")
    width = value_rows.shape[1] // count
    capacity = 2 * rows * routes.shape[1] // count
    bf16, f32 = jnp.bfloat16, jnp.float32
    dma = pltpu.SemaphoreType.DMA
    split = lambda weight: weight.reshape(sides, weight.shape[-2] // sides, weight.shape[-1])
    down, sdown = split(expert_down[0]), split(shared_down)
    weight_shape = (sides, cols, cols)
    slots = (count, capacity, cols)
    return pl.pallas_call(
        functools.partial(layer_kernel, count, capacity, (width // 2) ** (-0.5)),
        out_shape=jax.ShapeDtypeStruct((rows, cols), bf16),
        in_specs=[SMEM] + [VMEM] * 9 + [ANY] * 7,
        out_specs=VMEM,
        scratch_shapes=[
            pltpu.VMEM((count, rows + rows // 2, 2 * width), bf16),
            pltpu.VMEM((count, rows + rows // 2, 2 * width), bf16),
            pltpu.VMEM((count, 1, rows), jnp.int32),
            pltpu.VMEM((count, rows, 8), f32),
            pltpu.VMEM((count, 2, rows, 2 * width), bf16),
            pltpu.VMEM((count, width, rows), bf16),
            pltpu.VMEM((count, 4, rows), f32),
            pltpu.VMEM((count, 4, rows), f32),
            pltpu.VMEM((count, 4, width, rows), f32),
            pltpu.VMEM((count, rows // 2, 2 * width), bf16),
            pltpu.VMEM((rows, 128), f32),
        ]
        + [pltpu.VMEM(weight_shape, bf16)] * 5
        + [pltpu.VMEM((2, 2, cols, cols), bf16)] * 2
        + [
            pltpu.VMEM((count, rows // 2, 2 * width), bf16),
            pltpu.VMEM((sides, 2, rows // 2, cols), bf16),
            pltpu.VMEM((sides, 2, rows // 2, cols), bf16),
            pltpu.VMEM((sides, rows, cols), bf16),
            pltpu.VMEM((2, rows, cols), bf16),
            pltpu.VMEM((2, rows, cols), bf16),
            pltpu.VMEM((count, capacity, rows), bf16),
            pltpu.VMEM((sides,) + slots, bf16),
            pltpu.VMEM((sides,) + slots, bf16),
            pltpu.VMEM((2,) + slots, bf16),
            pltpu.VMEM((2,) + slots, bf16),
            pltpu.VMEM(slots, f32),
            pltpu.VMEM(slots, bf16),
            pltpu.VMEM(slots, bf16),
            pltpu.VMEM((rows, cols), f32),
            dma((9,)),
            dma((2, count)),
            dma((2, count)),
            dma((2, 2)),
            dma((2, 2)),
            dma((count,)),
            dma((count,)),
            dma((count + 4, 4)),
            dma((count + 4, 4)),
            dma((count + 1, 2)),
            dma((count + 1, 2)),
            dma((count,)),
            dma((count,)),
            dma((count,)),
            dma((count,)),
        ],
        compiler_params=pltpu.CompilerParams(
            collective_id=0, has_side_effects=True, vmem_limit_bytes=60 * 2**20
        ),
        name="layer",
    )(
        contrast_lambda,
        query_pairs,
        key_pairs,
        value_rows,
        doc_ids.reshape(1, rows),
        head_gain.reshape(1, width),
        stream,
        norm_gain.reshape(sides, 1, cols),
        routes.T,
        route_weights.T,
        split(out_proj),
        split(shared_gate),
        split(shared_up),
        split(expert_gate[0]),
        split(expert_up[0]),
        sdown,
        down,
    )


def choose(*args):
    query_pairs, value_rows, heads, stream = args[0], args[2], args[4].shape[0], args[6]
    count, sides = lax.axis_size("sp"), lax.axis_size("tp")
    width = value_rows.shape[1] // heads
    rows, cols = stream.shape
    hidden = {args[i].shape[-1] for i in (7, 11, 12, 13, 14, 15, 16)}
    fits = (
        heads == count
        and count & (count - 1) == 0
        and 8 <= count <= 128
        and sides == 4
        and 2 * width == 128
        and query_pairs.shape[1] == value_rows.shape[1] == cols
        and hidden == {cols}
        and all(args[i].shape[-2] == sides * cols for i in (7, 11, 12, 13, 14, 15, 16))
        and rows % 256 == 0
        and (2 * rows * args[9].shape[1]) % (128 * count) == 0
        and args[9].shape[1] == 2
    )
    return (head_per_device if fits else shards)(*args)


def solution(mesh):
    return jax.shard_map(
        choose,
        mesh=mesh,
        in_specs=(
            P("sp", "tp"),
            P("sp", "tp"),
            P("sp", "tp"),
            P("sp"),
            P("tp"),
            P(),
            P("sp", "tp"),
            P(None, "tp"),
            P(),
            P("sp", None),
            P("sp", None),
            P("sp", None, "tp"),
            P("sp", None, "tp"),
            P("sp", None, "tp"),
            P(None, "tp"),
            P(None, "tp"),
            P(None, "tp"),
        ),
        out_specs=P("sp", "tp"),
        check_vma=False,
    )
```

```python
import functools
import math

import jax
import jax.numpy as jnp
from jax import lax
from jax.experimental import pallas as pl
from jax.experimental.pallas import tpu as pltpu
from jax.sharding import PartitionSpec as P

epsilon = 1e-06
floor_score = -1e30


def add_columns(weight_rows, part_block):
    return jnp.dot(part_block, weight_rows, preferred_element_type=jnp.float32)


def shards(
    query_pairs,
    key_pairs,
    value_rows,
    doc_ids,
    contrast_lambda,
    head_gain,
    stream,
    out_proj,
    norm_gain,
    routes,
    route_weights,
    expert_gate,
    expert_up,
    expert_down,
    shared_gate,
    shared_up,
    shared_down,
):
    row_count = query_pairs.shape[0]
    local_heads = contrast_lambda.shape[0]
    key_width = query_pairs.shape[1] // (2 * local_heads)
    value_width = value_rows.shape[1] // local_heads
    scaling = key_width ** (-0.5)
    first_row = lax.axis_index("sp") * row_count
    query_pos = first_row + jnp.arange(row_count, dtype=jnp.int32)
    last_query = first_row + row_count - 1
    first_doc = doc_ids[0]
    query_split = query_pairs.reshape(row_count, local_heads, 2, key_width)

    def absorb_block(running, key_block, value_block, doc_block, key_start):
        best, denom, numer = running
        span_len = key_block.shape[0]
        key_pos = key_start + jnp.arange(span_len, dtype=jnp.int32)
        allowed = (key_pos[None, :] <= query_pos[:, None]) & (
            doc_block[None, :] == doc_ids[:, None]
        )
        scores = (
            jnp.einsum(
                "qhmd,khmd->hmqk",
                query_split,
                key_block.reshape(span_len, local_heads, 2, key_width),
                preferred_element_type=jnp.float32,
            )
            * scaling
        )
        scores = jnp.where(allowed, scores, floor_score)
        new_best = jnp.maximum(best, jnp.max(scores, axis=-1))
        weights = jnp.where(allowed, jnp.exp(scores - new_best[..., None]), 0.0)
        fade = jnp.exp(best - new_best)
        denom = denom * fade + jnp.sum(weights, axis=-1)
        numer = numer * fade[..., None] + jnp.einsum(
            "hmqk,khv->hmqv",
            weights.astype(jnp.bfloat16),
            value_block.reshape(span_len, local_heads, value_width),
            preferred_element_type=jnp.float32,
        )
        return (new_best, denom, numer)

    start_best = jnp.full((local_heads, 2, row_count), floor_score, jnp.float32)
    start_denom = jnp.zeros((local_heads, 2, row_count), jnp.float32)
    start_numer = jnp.zeros((local_heads, 2, row_count, value_width), jnp.float32)
    key_piece = lax.all_gather(key_pairs, "sp", axis=0, tiled=True)
    value_piece = lax.all_gather(value_rows, "sp", axis=0, tiled=True)
    doc_piece = lax.all_gather(doc_ids, "sp", axis=0, tiled=True)
    length = key_piece.shape[0]
    span_len = row_count * max(1, 512 // row_count)

    def one_span(span_index, carried):
        offset = span_index * span_len
        key_block = lax.dynamic_slice_in_dim(key_piece, offset, span_len, 0)
        value_block = lax.dynamic_slice_in_dim(value_piece, offset, span_len, 0)
        doc_block = lax.dynamic_slice_in_dim(doc_piece, offset, span_len, 0)
        needed = (offset <= last_query) & (doc_block[span_len - 1] >= first_doc)
        return lax.cond(
            needed,
            lambda held: absorb_block(held, key_block, value_block, doc_block, offset),
            lambda held: held,
            carried,
        )

    best, denom, numer = lax.fori_loop(
        0, length // span_len, one_span, (start_best, start_denom, start_numer)
    )
    heard = numer / denom[..., None]
    contrast = heard[:, 0] - contrast_lambda[:, None, None] * heard[:, 1]
    contrast = (
        contrast
        * lax.rsqrt(jnp.mean(contrast * contrast, axis=-1, keepdims=True) + epsilon)
        * head_gain
    )
    head_out = (
        jnp.transpose(contrast, (1, 0, 2))
        .reshape(row_count, local_heads * value_width)
        .astype(jnp.bfloat16)
    )
    projected = add_columns(out_proj, lax.all_gather(head_out, "tp", axis=1, tiled=True))
    hidden_cols = (stream.astype(jnp.float32) + projected).astype(jnp.bfloat16)
    hidden_rows = lax.all_gather(hidden_cols, "tp", axis=1, tiled=True)
    widened = hidden_rows.astype(jnp.float32)
    normed = (
        widened
        * lax.rsqrt(jnp.mean(widened * widened, axis=-1, keepdims=True) + epsilon)
        * norm_gain
    ).astype(jnp.bfloat16)
    shared_act = (
        jax.nn.silu(jnp.dot(normed, shared_gate, preferred_element_type=jnp.float32))
        * jnp.dot(normed, shared_up, preferred_element_type=jnp.float32)
    ).astype(jnp.bfloat16)
    shared_cols = add_columns(shared_down, lax.all_gather(shared_act, "tp", axis=1, tiled=True))
    expert_count = lax.axis_size("sp")
    route_count = routes.shape[1]
    capacity = 2 * row_count * route_count // expert_count
    flat_routes = routes.reshape(-1)
    hits = (flat_routes[:, None] == jnp.arange(expert_count, dtype=jnp.int32)[None, :]).astype(
        jnp.int32
    )
    position = jnp.sum(jnp.cumsum(hits, axis=0) * hits, axis=1) - 1
    target = flat_routes * capacity + position
    sources = jnp.arange(flat_routes.shape[0], dtype=jnp.int32) // route_count
    owner = jnp.zeros((expert_count * capacity,), jnp.int32).at[target].set(sources)
    outgoing = normed[owner].reshape(expert_count, capacity, normed.shape[1])
    gate_cols = expert_gate[0]
    up_cols = expert_up[0]
    down_cols = expert_down[0]
    slice_width = outgoing.shape[2] // lax.axis_size("tp")
    own_slice = lax.dynamic_slice_in_dim(
        outgoing, lax.axis_index("tp") * slice_width, slice_width, 2
    )
    arrived = lax.all_to_all(own_slice, "sp", split_axis=0, concat_axis=0, tiled=True)
    apply_arrived = lax.all_gather(arrived, "tp", axis=2, tiled=True)
    gated = jnp.einsum("snd,df->snf", apply_arrived, gate_cols, preferred_element_type=jnp.float32)
    lifted = jnp.einsum("snd,df->snf", apply_arrived, up_cols, preferred_element_type=jnp.float32)
    expert_act = (jax.nn.silu(gated) * lifted).astype(jnp.bfloat16)
    expert_out = add_columns(
        down_cols, lax.all_gather(expert_act, "tp", axis=2, tiled=True)
    ).astype(jnp.bfloat16)
    returned = lax.all_to_all(expert_out, "sp", split_axis=0, concat_axis=0, tiled=True)
    flat_back = returned.reshape(expert_count * capacity, returned.shape[2])
    picked = (
        flat_back[target].reshape(row_count, route_count, returned.shape[2]).astype(jnp.float32)
    )
    routed = jnp.sum(picked * route_weights[:, :, None], axis=1)
    return (hidden_cols.astype(jnp.float32) + shared_cols + routed).astype(jnp.bfloat16)


MESH_ID = pl.DeviceIdType.MESH
VMEM = pl.BlockSpec(memory_space=pltpu.VMEM)
ANY = pl.BlockSpec(memory_space=pl.ANY)
SMEM = pl.BlockSpec(memory_space=pltpu.SMEM)


def flip(index, mask, size):
    out, bit = 0, 1
    while bit < size:
        out = out + bit * lax.rem(lax.div(index, bit) + lax.div(mask, bit), 2)
        bit *= 2
    return out


def remote(src, dst, send, recv, device):
    return pltpu.make_async_remote_copy(
        src_ref=src,
        dst_ref=dst,
        send_sem=send,
        recv_sem=recv,
        device_id=device,
        device_id_type=MESH_ID,
    )


def fold_axes(me, col):
    core = lax.rem(me, 2)
    return flip(col, 2 - core, 4), flip(col, 1 + core, 4), flip(col, jnp.int32(3), 4)


def layer_kernel(
    count,
    capacity,
    scaling,
    lam_ref,
    q_ref,
    k_ref,
    v_ref,
    doc_ref,
    head_gain_ref,
    stream_ref,
    gain_ref,
    routes_ref,
    weight_ref,
    proj_hbm,
    sgate_hbm,
    sup_hbm,
    gate_hbm,
    up_hbm,
    sdown_hbm,
    down_hbm,
    out_ref,
    pack,
    qkv,
    docs,
    doc_cols,
    queries,
    turned,
    best_ref,
    denom_ref,
    numer_ref,
    head_out,
    portions,
    proj,
    sgate,
    sup,
    gate,
    up,
    sdown,
    down,
    held,
    head_buf,
    hidden_buf,
    normed,
    shared_buf,
    shared_part,
    onehot,
    outgoing,
    rows_in,
    acts,
    parts,
    kept,
    made,
    back,
    made_two,
    shared_cols,
    load_sem,
    xsend,
    xrecv,
    wsend,
    wrecv,
    hsend,
    hrecv,
    gsend,
    grecv,
    fsend,
    frecv,
    zsend,
    zrecv,
    rsend,
    rrecv,
):
    me, col = lax.axis_index("sp"), lax.axis_index("tp")
    rows, cols = stream_ref.shape
    half = rows // 2
    width = head_gain_ref.shape[1]
    key_width = width // 2
    f32 = jnp.float32
    meet, fold, across = fold_axes(me, col)
    loads = [
        pltpu.make_async_copy(a, b, load_sem.at[i])
        for i, (a, b) in enumerate(
            (
                (proj_hbm, proj),
                (sgate_hbm, sgate),
                (sup_hbm, sup),
                (gate_hbm, gate),
                (up_hbm, up),
                (sdown_hbm.at[col], sdown.at[0, 0]),
                (sdown_hbm.at[meet], sdown.at[0, 1]),
                (down_hbm.at[col], down.at[0, 0]),
                (down_hbm.at[meet], down.at[0, 1]),
            )
        )
    ]
    for load in loads:
        load.start()
    side = [flip(col, jnp.int32(j), 4) for j in range(4)]
    peer = lambda k: (flip(me, k, count), col)
    near_x, near_y = (me, side[1]), (me, side[2])
    friends = [peer(jnp.int32(k)) for k in range(1, count)] + [near_x, near_y]
    barrier = pltpu.get_barrier_semaphore()
    for device in friends:
        pl.semaphore_signal(barrier, inc=1, device_id=device, device_id_type=MESH_ID)
    for h in range(count):
        cut = slice(h * width, (h + 1) * width)
        pack[h, :rows, :] = jnp.concatenate([q_ref[:, cut], k_ref[:, cut]], axis=1)
        pack[h, rows:, :] = jnp.concatenate([v_ref[:half, cut], v_ref[half:, cut]], axis=1)
    pl.semaphore_wait(barrier, len(friends))

    def direct(buf, row, index):
        own = buf.at[(0,) + index]
        return (
            remote(own, buf.at[(1,) + index], gsend.at[row, 0], grecv.at[row, 0], near_x),
            remote(own, buf.at[(2,) + index], gsend.at[row, 1], grecv.at[row, 1], near_y),
        )

    def relays(buf, row, index):
        middle = buf.shape[-2] // 2
        top, low = pl.ds(0, middle), pl.ds(middle, middle)
        return (
            remote(
                buf.at[(1,) + index + (top,)], buf.at[(3,) + index + (top,)],
                gsend.at[row, 2], grecv.at[row, 2], near_y,
            ),
            remote(
                buf.at[(2,) + index + (low,)], buf.at[(3,) + index + (low,)],
                gsend.at[row, 3], grecv.at[row, 3], near_x,
            ),
        )

    def offer(buf, row, index=()):
        for copy in direct(buf, row, index):
            copy.start()

    def pass_on(buf, row, index=()):
        for first, second in zip(direct(buf, row, index), relays(buf, row, index)):
            first.wait_recv()
            second.start()

    def finish(buf, row, index=()):
        for copy in relays(buf, row, index):
            copy.wait_recv()

    def drain(buf, row, index=()):
        for copy in direct(buf, row, index) + relays(buf, row, index):
            copy.wait_send()

    def join(buf, row, index=()):
        own, other = buf.at[(0,) + index], buf.at[(1,) + index]
        return remote(own, other, fsend.at[row, 0], frecv.at[row, 0], (me, meet))

    def hand_over(buf, row, index=()):
        own, other = buf.at[(0,) + index], buf.at[(1,) + index]
        return remote(own, other, fsend.at[row, 1], frecv.at[row, 1], (me, fold))

    row_head, row_hidden, row_shared = count, count + count // 2, count

    def exchange(k):
        there = peer(k)
        return (
            remote(doc_ref, docs.at[me], xsend.at[0, k], xrecv.at[0, k], there),
            remote(pack.at[there[0]], qkv.at[me], xsend.at[1, k], xrecv.at[1, k], there),
        )

    def head_copy(k):
        there = peer(k)
        return remote(head_out.at[there[0]], held.at[me], hsend.at[k], hrecv.at[k], there)

    swaps = [
        remote(src.at[quarter], dst.at[1, i], wsend.at[j, i], wrecv.at[j, i], (me, fold))
        for j, (src, dst) in enumerate(((down_hbm, down), (sdown_hbm, sdown)))
        for i, quarter in enumerate((fold, across))
    ]
    for k in range(1, count):
        for copy in exchange(jnp.int32(k)):
            copy.start()
    for swap in swaps:
        swap.start()
    qkv[me] = pack[me]
    docs[me] = doc_ref[...]
    best_ref[...] = jnp.full(best_ref.shape, floor_score, f32)
    denom_ref[...] = jnp.zeros(denom_ref.shape, f32)
    numer_ref[...] = jnp.zeros(numer_ref.shape, f32)

    near = routes_ref[...] ^ me
    lane = lax.broadcasted_iota(jnp.int32, (128, rows), 0)
    hits = [near[j : j + 1, :] == lane for j in range(2)]
    present = hits[0] | hits[1]
    before = (
        lax.broadcasted_iota(jnp.int32, (rows, rows), 0)
        < lax.broadcasted_iota(jnp.int32, (rows, rows), 1)
    )
    place = jnp.dot(
        present.astype(f32).astype(jnp.bfloat16),
        before.astype(f32).astype(jnp.bfloat16),
        preferred_element_type=f32,
    )
    place = jnp.where(present, place, -1.0)
    slot = lax.broadcasted_iota(jnp.int32, (capacity, rows), 0).astype(f32)
    for k in range(count):
        onehot[k] = (slot == place[k : k + 1, :]).astype(f32).astype(jnp.bfloat16)
    portion = jnp.where(hits[0], weight_ref[0:1, :], 0.0) + jnp.where(
        hits[1], weight_ref[1:2, :], 0.0
    )
    portions[...] = jnp.transpose(portion)

    weight = lam_ref[me]
    gains = jnp.concatenate([head_gain_ref[...], head_gain_ref[...]], axis=1)
    factor = scaling * math.log2(math.e)
    lanes = lax.broadcasted_iota(jnp.int32, (rows, 2 * width), 1)

    def conclude(k):
        b = flip(me, k, count)
        heard = []
        for m in range(2):
            bests = [best_ref[b, pl.ds(2 * part + m, 1), :] for part in range(2)]
            top = jnp.maximum(*bests)
            fades = [jnp.exp2(best - top) for best in bests]
            denom, numer = [
                first * fades[0] + second * fades[1]
                for first, second in (
                    [denom_ref[b, pl.ds(2 * part + m, 1), :] for part in range(2)],
                    [numer_ref[b, 2 * part + m] for part in range(2)],
                )
            ]
            heard.append(numer / denom)
        contrast = heard[0] - weight * heard[1]
        contrast = contrast * lax.rsqrt(
            jnp.mean(contrast * contrast, axis=0, keepdims=True) + epsilon
        )
        stacked = jnp.concatenate([contrast[:, :half], contrast[:, half:]], axis=0)
        head_out[b] = (jnp.transpose(stacked) * gains).astype(jnp.bfloat16)

        @pl.when(k > 0)
        def _():
            head_copy(k).start()

    layer_of = lax.div(me, 2)
    lower = me < count // 2

    @pl.loop(0, count)
    def _(i):
        j = flip(me, i, count)

        @pl.when(i > 0)
        def _():
            for copy in exchange(i):
                copy.wait_recv()

        values = jnp.transpose(qkv[j, rows:, :].astype(f32)).astype(jnp.bfloat16)
        turned[j] = jnp.concatenate([values[:width], values[width:]], axis=1)
        moved = pltpu.roll(qkv[j, :rows, :].astype(f32), width, 1)
        for m in range(2):
            begin = width + m * key_width
            inside = (lanes >= begin) & (lanes < begin + key_width)
            queries[j, m] = jnp.where(inside, moved, 0.0).astype(jnp.bfloat16)
        doc_cols[j] = jnp.transpose(jnp.broadcast_to(docs[j].astype(f32), (8, rows)))

        def pair_of_tiles(step, carried):
            step = lax.div(i, 2) - step
            ahead = lax.broadcasted_iota(jnp.int32, (rows, rows), 0) - lax.broadcasted_iota(
                jnp.int32, (rows, rows), 1
            )
            tiles = []
            for part in range(2):
                second = 2 * step + part
                other = flip(me, jnp.minimum(second, i), count)
                q, k = jnp.maximum(j, other), jnp.minimum(j, other)
                limit = jnp.where(second <= i, (q - k) * rows, -rows)
                allowed = (ahead <= limit) & (doc_cols[k][:, 0:1] == docs[q].astype(f32))
                tiles.append((q, k, allowed))
            scores = [
                [
                    jnp.where(
                        allowed,
                        lax.dot_general(
                            qkv[k, :rows, :], queries[q, m], (((1,), (1,)), ((), ())),
                            preferred_element_type=f32,
                        )
                        * factor,
                        floor_score,
                    )
                    for m in range(2)
                ]
                for q, k, allowed in tiles
            ]
            for part, (q, k, _) in enumerate(tiles):
                for m in range(2):
                    row = pl.ds(2 * part + m, 1)
                    tile = scores[part][m]
                    best = best_ref[q, row, :]
                    new_best = jnp.maximum(best, jnp.max(tile, axis=0, keepdims=True))
                    fade = jnp.exp2(best - new_best)
                    weights = jnp.exp2(tile - new_best)
                    best_ref[q, row, :] = new_best
                    denom_ref[q, row, :] = denom_ref[q, row, :] * fade + jnp.sum(
                        weights, axis=0, keepdims=True
                    )
                    numer_ref[q, 2 * part + m] = numer_ref[q, 2 * part + m] * fade + jnp.dot(
                        turned[k], weights.astype(jnp.bfloat16), preferred_element_type=f32
                    )
            return carried

        pairs = lax.div(i, 2) + 1
        early = jnp.where(i == count - 1, count // 4, pairs)
        lax.fori_loop(0, early, pair_of_tiles, 0)

        @pl.when(i == count - 1)
        def _():
            @pl.loop(count // 2, count)
            def _(n):
                @pl.when((n < count - 1) | jnp.logical_not(lower))
                def _():
                    conclude(n)

        lax.fori_loop(early, pairs, pair_of_tiles, 0)

    @pl.when(lower)
    def _():
        conclude(jnp.int32(count - 1))

    @pl.loop(0, count // 2)
    def _(n):
        conclude(count // 2 - 1 - n)

    held[me] = head_out[me]
    @pl.loop(0, count // 2)
    def _(q):
        for k in range(2):
            @pl.when(2 * q + k > 0)
            def _():
                head_copy(2 * q + k).wait_recv()

        pair = flip(layer_of, q, count // 2)
        first, second = held[2 * pair], held[2 * pair + 1]
        for h in range(2):
            part = slice(h * width, (h + 1) * width)
            span = slice(h * half, (h + 1) * half)
            head_buf[0, q, span, :] = jnp.concatenate([first[:, part], second[:, part]], axis=1)
        offer(head_buf, row_head + q, (q,))

        @pl.when(q > 0)
        def _():
            pass_on(head_buf, row_head + q - 1, (q - 1,))

    pass_on(head_buf, row_head + count // 2 - 1, (count // 2 - 1,))
    loads[0].wait()

    def projected(j):
        blocks = [head_buf[j, flip(layer_of, jnp.int32(p), count // 2)] for p in range(count // 2)]
        block = jnp.concatenate(blocks, axis=1)
        return jnp.dot(block, proj[side[j]], preferred_element_type=f32)

    total = projected(0) + projected(1) + projected(2)
    for q in range(count // 2):
        finish(head_buf, row_head + q, (q,))
    total = total + projected(3)
    for h in range(2):
        span = slice(h * half, (h + 1) * half)
        hidden_buf[0, h] = (stream_ref[span, :].astype(f32) + total[span]).astype(jnp.bfloat16)
        offer(hidden_buf, row_hidden + h, (h,))

    def dispatch_far(k):
        return remote(outgoing.at[0, k], rows_in.at[0, k], zsend.at[k], zrecv.at[k], peer(k))

    def dispatch_near(k):
        return remote(outgoing.at[:, k], rows_in.at[:, k], zsend.at[k], zrecv.at[k], peer(k))

    def chosen(k, j):
        block = hidden_buf[j].reshape(rows, cols)
        return jnp.dot(onehot[k], block, preferred_element_type=f32).astype(jnp.bfloat16)

    for k in range(4, count):
        outgoing[0, k] = chosen(k, 0)
        dispatch_far(jnp.int32(k)).start()
    for h in range(2):
        pass_on(hidden_buf, row_hidden + h, (h,))

    def scaled(blocks):
        wide = [block.astype(f32) for block in blocks]
        squares = wide[0] * wide[0]
        for block in wide[1:]:
            squares = squares + block * block
        scale = lax.rsqrt(jnp.sum(squares, axis=1, keepdims=True) / (4 * cols) + epsilon)
        return [
            (block * scale * gain_ref[side[j]]).astype(jnp.bfloat16)
            for j, block in enumerate(wide)
        ]

    def gated_pair(blocks, first, second):
        gated, lifted = [
            sum(jnp.dot(block, w[side[j]], preferred_element_type=f32) for j, block in enumerate(blocks))
            for w in (first, second)
        ]
        return (jax.nn.silu(gated) * lifted).astype(jnp.bfloat16)

    for h in range(2):
        finish(hidden_buf, row_hidden + h, (h,))
    for j in range(4):
        outgoing[j, 1] = chosen(1, j)
    dispatch_near(jnp.int32(1)).start()
    for j in range(4):
        rows_in[j, 0] = chosen(0, j)
    for load in loads[1:]:
        load.wait()

    def first_half(k):
        acts[0, k] = gated_pair(scaled([rows_in[j, k] for j in range(4)]), gate, up)
        join(acts, k, (k,)).start()

    first_half(0)
    for h in range(2):
        span = slice(h * half, (h + 1) * half)
        for j, block in enumerate(scaled([hidden_buf[j, h] for j in range(4)])):
            normed[j, span, :] = block
    shared_buf[0] = gated_pair([normed[j] for j in range(4)], sgate, sup)
    join(shared_buf, row_shared).start()
    dispatch_near(jnp.int32(1)).wait_recv()
    for swap in swaps:
        swap.wait_recv()
    dispatch_far(jnp.int32(4)).wait_recv()
    offer(rows_in, 4, (4,))

    def give_back(k):
        return remote(made.at[k], back.at[k], rsend.at[k], rrecv.at[k], peer(k))

    def turn(p):
        later = jnp.where(p < count - 2, p + 2, p - count + 4)
        return jnp.where(p < 2, p, later)

    def second_half(buf, second, index=()):
        return [
            jnp.dot(buf[(0,) + index], second[c, 0], preferred_element_type=f32)
            + jnp.dot(buf[(1,) + index], second[c, 1], preferred_element_type=f32)
            for c in range(2)
        ]

    def scattered(k, block):
        picked = lax.dot_general(
            onehot[k], block, (((0,), (0,)), ((), ())), preferred_element_type=f32
        )
        return portions[:, k : k + 1] * picked

    @pl.loop(0, count + 1)
    def _(i):
        @pl.when(i < 2)
        def _():
            for j in range(4):
                block = hidden_buf[j].reshape(rows, cols)
                outgoing[j, i + 2] = jnp.dot(
                    onehot[i + 2], block, preferred_element_type=f32
                ).astype(jnp.bfloat16)
            dispatch_near(i + 2).start()

        @pl.when(i < count - 5)
        def _():
            dispatch_far(i + 5).wait_recv()
            offer(rows_in, i + 5, (i + 5,))

        @pl.when(i < count - 4)
        def _():
            pass_on(rows_in, i + 4, (i + 4,))

        @pl.when((i >= 1) & (i < count - 3))
        def _():
            finish(rows_in, i + 3, (i + 3,))

        @pl.when((i >= count - 3) & (i < count - 1))
        def _():
            dispatch_near(turn(i + 1)).wait_recv()

        @pl.when(i < count - 1)
        def _():
            first_half(turn(i + 1))

        @pl.when(i == 0)
        def _():
            join(acts, 0, (0,)).wait_recv()
            for c, block in enumerate(second_half(acts, down, (0,))):
                made_two[c] = block.astype(jnp.bfloat16)

        @pl.when(i == 1)
        def _():
            join(shared_buf, row_shared).wait_recv()
            for c, block in enumerate(second_half(shared_buf, sdown)):
                shared_cols[c] = block

        @pl.when((i >= 1) & (i < count))
        def _():
            k = turn(i)
            join(acts, k, (k,)).wait_recv()
            own, other = second_half(acts, down, (k,))
            parts[0, k] = other.astype(jnp.bfloat16)
            hand_over(parts, k, (k,)).start()
            kept[k] = own

        @pl.when(i == 2)
        def _():
            for c in range(2):
                shared_cols[c] = shared_cols[c] + scattered(0, made_two[c])
            shared_part[0] = shared_cols[1].astype(jnp.bfloat16)

        @pl.when(i == count - 1)
        def _():
            hand_over(shared_part, row_shared).start()

        @pl.when(i >= 2)
        def _():
            k = turn(i - 1)
            hand_over(parts, k, (k,)).wait_recv()
            made[k] = (kept[k] + parts[1, k].astype(f32)).astype(jnp.bfloat16)
            give_back(k).start()

    total = shared_cols[0]
    for k in [1] + list(range(4, count)) + [2, 3]:
        give_back(jnp.int32(k)).wait_recv()
        total = total + scattered(k, back[k])
    hand_over(shared_part, row_shared).wait_recv()
    total = total + shared_part[1].astype(f32)
    for h in range(2):
        span = slice(h * half, (h + 1) * half)
        out_ref[span, :] = (hidden_buf[0, h].astype(f32) + total[span]).astype(jnp.bfloat16)

    for swap in swaps:
        swap.wait_send()
    for q in range(count // 2):
        drain(head_buf, row_head + q, (q,))
    for h in range(2):
        drain(hidden_buf, row_hidden + h, (h,))
    join(shared_buf, row_shared).wait_send()
    hand_over(shared_part, row_shared).wait_send()

    @pl.loop(4, count)
    def _(k):
        drain(rows_in, k, (k,))
        dispatch_far(k).wait_send()

    @pl.loop(1, 4)
    def _(k):
        dispatch_near(k).wait_send()

    @pl.loop(1, count)
    def _(k):
        head_copy(k).wait_send()
        for copy in exchange(k):
            copy.wait_send()

    @pl.loop(0, count)
    def _(k):
        join(acts, k, (k,)).wait_send()

        @pl.when(k > 0)
        def _():
            hand_over(parts, k, (k,)).wait_send()
            give_back(k).wait_send()


def head_per_device(
    query_pairs,
    key_pairs,
    value_rows,
    doc_ids,
    contrast_lambda,
    head_gain,
    stream,
    out_proj,
    norm_gain,
    routes,
    route_weights,
    expert_gate,
    expert_up,
    expert_down,
    shared_gate,
    shared_up,
    shared_down,
):
    rows, cols = stream.shape
    count, sides = lax.axis_size("sp"), lax.axis_size("tp")
    width = value_rows.shape[1] // count
    capacity = 2 * rows * routes.shape[1] // count
    bf16, f32 = jnp.bfloat16, jnp.float32
    dma = pltpu.SemaphoreType.DMA
    split = lambda weight: weight.reshape(sides, weight.shape[-2] // sides, weight.shape[-1])
    down, sdown = split(expert_down[0]), split(shared_down)
    weight_shape = (sides, cols, cols)
    slots = (count, capacity, cols)
    return pl.pallas_call(
        functools.partial(layer_kernel, count, capacity, (width // 2) ** (-0.5)),
        out_shape=jax.ShapeDtypeStruct((rows, cols), bf16),
        in_specs=[SMEM] + [VMEM] * 9 + [ANY] * 7,
        out_specs=VMEM,
        scratch_shapes=[
            pltpu.VMEM((count, rows + rows // 2, 2 * width), bf16),
            pltpu.VMEM((count, rows + rows // 2, 2 * width), bf16),
            pltpu.VMEM((count, 1, rows), jnp.int32),
            pltpu.VMEM((count, rows, 8), f32),
            pltpu.VMEM((count, 2, rows, 2 * width), bf16),
            pltpu.VMEM((count, width, rows), bf16),
            pltpu.VMEM((count, 4, rows), f32),
            pltpu.VMEM((count, 4, rows), f32),
            pltpu.VMEM((count, 4, width, rows), f32),
            pltpu.VMEM((count, rows // 2, 2 * width), bf16),
            pltpu.VMEM((rows, 128), f32),
        ]
        + [pltpu.VMEM(weight_shape, bf16)] * 5
        + [pltpu.VMEM((2, 2, cols, cols), bf16)] * 2
        + [
            pltpu.VMEM((count, rows // 2, 2 * width), bf16),
            pltpu.VMEM((sides, count // 2, rows, cols // (count // 2)), bf16),
            pltpu.VMEM((sides, 2, rows // 2, cols), bf16),
            pltpu.VMEM((sides, rows, cols), bf16),
            pltpu.VMEM((2, rows, cols), bf16),
            pltpu.VMEM((2, rows, cols), bf16),
            pltpu.VMEM((count, capacity, rows), bf16),
            pltpu.VMEM((sides,) + slots, bf16),
            pltpu.VMEM((sides,) + slots, bf16),
            pltpu.VMEM((2,) + slots, bf16),
            pltpu.VMEM((2,) + slots, bf16),
            pltpu.VMEM(slots, f32),
            pltpu.VMEM(slots, bf16),
            pltpu.VMEM(slots, bf16),
            pltpu.VMEM((2, capacity, cols), bf16),
            pltpu.VMEM((2, rows, cols), f32),
            dma((9,)),
            dma((2, count)),
            dma((2, count)),
            dma((2, 2)),
            dma((2, 2)),
            dma((count,)),
            dma((count,)),
            dma((count + count // 2 + 2, 4)),
            dma((count + count // 2 + 2, 4)),
            dma((count + 1, 2)),
            dma((count + 1, 2)),
            dma((count,)),
            dma((count,)),
            dma((count,)),
            dma((count,)),
        ],
        compiler_params=pltpu.CompilerParams(
            collective_id=0, has_side_effects=True, vmem_limit_bytes=60 * 2**20
        ),
        name="layer",
    )(
        contrast_lambda,
        query_pairs,
        key_pairs,
        value_rows,
        doc_ids.reshape(1, rows),
        head_gain.reshape(1, width),
        stream,
        norm_gain.reshape(sides, 1, cols),
        routes.T,
        route_weights.T,
        split(out_proj),
        split(shared_gate),
        split(shared_up),
        split(expert_gate[0]),
        split(expert_up[0]),
        sdown,
        down,
    )


def choose(*args):
    query_pairs, value_rows, heads, stream = args[0], args[2], args[4].shape[0], args[6]
    count, sides = lax.axis_size("sp"), lax.axis_size("tp")
    width = value_rows.shape[1] // heads
    rows, cols = stream.shape
    hidden = {args[i].shape[-1] for i in (7, 11, 12, 13, 14, 15, 16)}
    fits = (
        heads == count
        and count & (count - 1) == 0
        and 8 <= count <= 128
        and sides == 4
        and 2 * width == 128
        and query_pairs.shape[1] == value_rows.shape[1] == cols
        and hidden == {cols}
        and all(args[i].shape[-2] == sides * cols for i in (7, 11, 12, 13, 14, 15, 16))
        and rows % 256 == 0
        and (2 * rows * args[9].shape[1]) % (128 * count) == 0
        and args[9].shape[1] == 2
    )
    return (head_per_device if fits else shards)(*args)


def solution(mesh):
    return jax.shard_map(
        choose,
        mesh=mesh,
        in_specs=(
            P("sp", "tp"),
            P("sp", "tp"),
            P("sp", "tp"),
            P("sp"),
            P("tp"),
            P(),
            P("sp", "tp"),
            P(None, "tp"),
            P(),
            P("sp", None),
            P("sp", None),
            P("sp", None, "tp"),
            P("sp", None, "tp"),
            P("sp", None, "tp"),
            P(None, "tp"),
            P(None, "tp"),
            P(None, "tp"),
        ),
        out_specs=P("sp", "tp"),
        check_vma=False,
    )
```

```python
import functools
import math

import jax
import jax.numpy as jnp
from jax import lax
from jax.experimental import pallas as pl
from jax.experimental.pallas import tpu as pltpu
from jax.sharding import PartitionSpec as P

epsilon = 1e-06
floor_score = -1e30


def add_columns(weight_rows, part_block):
    return jnp.dot(part_block, weight_rows, preferred_element_type=jnp.float32)


def shards(
    query_pairs,
    key_pairs,
    value_rows,
    doc_ids,
    contrast_lambda,
    head_gain,
    stream,
    out_proj,
    norm_gain,
    routes,
    route_weights,
    expert_gate,
    expert_up,
    expert_down,
    shared_gate,
    shared_up,
    shared_down,
):
    row_count = query_pairs.shape[0]
    local_heads = contrast_lambda.shape[0]
    key_width = query_pairs.shape[1] // (2 * local_heads)
    value_width = value_rows.shape[1] // local_heads
    scaling = key_width ** (-0.5)
    first_row = lax.axis_index("sp") * row_count
    query_pos = first_row + jnp.arange(row_count, dtype=jnp.int32)
    last_query = first_row + row_count - 1
    first_doc = doc_ids[0]
    query_split = query_pairs.reshape(row_count, local_heads, 2, key_width)

    def absorb_block(running, key_block, value_block, doc_block, key_start):
        best, denom, numer = running
        span_len = key_block.shape[0]
        key_pos = key_start + jnp.arange(span_len, dtype=jnp.int32)
        allowed = (key_pos[None, :] <= query_pos[:, None]) & (
            doc_block[None, :] == doc_ids[:, None]
        )
        scores = (
            jnp.einsum(
                "qhmd,khmd->hmqk",
                query_split,
                key_block.reshape(span_len, local_heads, 2, key_width),
                preferred_element_type=jnp.float32,
            )
            * scaling
        )
        scores = jnp.where(allowed, scores, floor_score)
        new_best = jnp.maximum(best, jnp.max(scores, axis=-1))
        weights = jnp.where(allowed, jnp.exp(scores - new_best[..., None]), 0.0)
        fade = jnp.exp(best - new_best)
        denom = denom * fade + jnp.sum(weights, axis=-1)
        numer = numer * fade[..., None] + jnp.einsum(
            "hmqk,khv->hmqv",
            weights.astype(jnp.bfloat16),
            value_block.reshape(span_len, local_heads, value_width),
            preferred_element_type=jnp.float32,
        )
        return (new_best, denom, numer)

    start_best = jnp.full((local_heads, 2, row_count), floor_score, jnp.float32)
    start_denom = jnp.zeros((local_heads, 2, row_count), jnp.float32)
    start_numer = jnp.zeros((local_heads, 2, row_count, value_width), jnp.float32)
    key_piece = lax.all_gather(key_pairs, "sp", axis=0, tiled=True)
    value_piece = lax.all_gather(value_rows, "sp", axis=0, tiled=True)
    doc_piece = lax.all_gather(doc_ids, "sp", axis=0, tiled=True)
    length = key_piece.shape[0]
    span_len = row_count * max(1, 512 // row_count)

    def one_span(span_index, carried):
        offset = span_index * span_len
        key_block = lax.dynamic_slice_in_dim(key_piece, offset, span_len, 0)
        value_block = lax.dynamic_slice_in_dim(value_piece, offset, span_len, 0)
        doc_block = lax.dynamic_slice_in_dim(doc_piece, offset, span_len, 0)
        needed = (offset <= last_query) & (doc_block[span_len - 1] >= first_doc)
        return lax.cond(
            needed,
            lambda held: absorb_block(held, key_block, value_block, doc_block, offset),
            lambda held: held,
            carried,
        )

    best, denom, numer = lax.fori_loop(
        0, length // span_len, one_span, (start_best, start_denom, start_numer)
    )
    heard = numer / denom[..., None]
    contrast = heard[:, 0] - contrast_lambda[:, None, None] * heard[:, 1]
    contrast = (
        contrast
        * lax.rsqrt(jnp.mean(contrast * contrast, axis=-1, keepdims=True) + epsilon)
        * head_gain
    )
    head_out = (
        jnp.transpose(contrast, (1, 0, 2))
        .reshape(row_count, local_heads * value_width)
        .astype(jnp.bfloat16)
    )
    projected = add_columns(out_proj, lax.all_gather(head_out, "tp", axis=1, tiled=True))
    hidden_cols = (stream.astype(jnp.float32) + projected).astype(jnp.bfloat16)
    hidden_rows = lax.all_gather(hidden_cols, "tp", axis=1, tiled=True)
    widened = hidden_rows.astype(jnp.float32)
    normed = (
        widened
        * lax.rsqrt(jnp.mean(widened * widened, axis=-1, keepdims=True) + epsilon)
        * norm_gain
    ).astype(jnp.bfloat16)
    shared_act = (
        jax.nn.silu(jnp.dot(normed, shared_gate, preferred_element_type=jnp.float32))
        * jnp.dot(normed, shared_up, preferred_element_type=jnp.float32)
    ).astype(jnp.bfloat16)
    shared_cols = add_columns(shared_down, lax.all_gather(shared_act, "tp", axis=1, tiled=True))
    expert_count = lax.axis_size("sp")
    route_count = routes.shape[1]
    capacity = 2 * row_count * route_count // expert_count
    flat_routes = routes.reshape(-1)
    hits = (flat_routes[:, None] == jnp.arange(expert_count, dtype=jnp.int32)[None, :]).astype(
        jnp.int32
    )
    position = jnp.sum(jnp.cumsum(hits, axis=0) * hits, axis=1) - 1
    target = flat_routes * capacity + position
    sources = jnp.arange(flat_routes.shape[0], dtype=jnp.int32) // route_count
    owner = jnp.zeros((expert_count * capacity,), jnp.int32).at[target].set(sources)
    outgoing = normed[owner].reshape(expert_count, capacity, normed.shape[1])
    gate_cols = expert_gate[0]
    up_cols = expert_up[0]
    down_cols = expert_down[0]
    slice_width = outgoing.shape[2] // lax.axis_size("tp")
    own_slice = lax.dynamic_slice_in_dim(
        outgoing, lax.axis_index("tp") * slice_width, slice_width, 2
    )
    arrived = lax.all_to_all(own_slice, "sp", split_axis=0, concat_axis=0, tiled=True)
    apply_arrived = lax.all_gather(arrived, "tp", axis=2, tiled=True)
    gated = jnp.einsum("snd,df->snf", apply_arrived, gate_cols, preferred_element_type=jnp.float32)
    lifted = jnp.einsum("snd,df->snf", apply_arrived, up_cols, preferred_element_type=jnp.float32)
    expert_act = (jax.nn.silu(gated) * lifted).astype(jnp.bfloat16)
    expert_out = add_columns(
        down_cols, lax.all_gather(expert_act, "tp", axis=2, tiled=True)
    ).astype(jnp.bfloat16)
    returned = lax.all_to_all(expert_out, "sp", split_axis=0, concat_axis=0, tiled=True)
    flat_back = returned.reshape(expert_count * capacity, returned.shape[2])
    picked = (
        flat_back[target].reshape(row_count, route_count, returned.shape[2]).astype(jnp.float32)
    )
    routed = jnp.sum(picked * route_weights[:, :, None], axis=1)
    return (hidden_cols.astype(jnp.float32) + shared_cols + routed).astype(jnp.bfloat16)


MESH_ID = pl.DeviceIdType.MESH
VMEM = pl.BlockSpec(memory_space=pltpu.VMEM)
ANY = pl.BlockSpec(memory_space=pl.ANY)
SMEM = pl.BlockSpec(memory_space=pltpu.SMEM)


def flip(index, mask, size):
    out, bit = 0, 1
    while bit < size:
        out = out + bit * lax.rem(lax.div(index, bit) + lax.div(mask, bit), 2)
        bit *= 2
    return out


def remote(src, dst, send, recv, device):
    return pltpu.make_async_remote_copy(
        src_ref=src,
        dst_ref=dst,
        send_sem=send,
        recv_sem=recv,
        device_id=device,
        device_id_type=MESH_ID,
    )


def fold_axes(me, col):
    core = lax.rem(me, 2)
    return flip(col, 2 - core, 4), flip(col, 1 + core, 4), flip(col, jnp.int32(3), 4)


def layer_kernel(
    count,
    capacity,
    scaling,
    lam_ref,
    q_ref,
    k_ref,
    v_ref,
    doc_ref,
    head_gain_ref,
    stream_ref,
    gain_ref,
    routes_ref,
    weight_ref,
    proj_hbm,
    sgate_hbm,
    sup_hbm,
    gate_hbm,
    up_hbm,
    sdown_hbm,
    down_hbm,
    out_ref,
    pack,
    qkv,
    docs,
    doc_cols,
    queries,
    turned,
    best_ref,
    denom_ref,
    numer_ref,
    head_out,
    portions,
    proj,
    sgate,
    sup,
    gate,
    up,
    sdown,
    down,
    held,
    head_buf,
    hidden_buf,
    normed,
    shared_buf,
    shared_part,
    onehot,
    outgoing,
    rows_in,
    acts,
    parts,
    kept,
    made,
    back,
    made_two,
    shared_cols,
    load_sem,
    xsend,
    xrecv,
    wsend,
    wrecv,
    hsend,
    hrecv,
    gsend,
    grecv,
    fsend,
    frecv,
    zsend,
    zrecv,
    rsend,
    rrecv,
):
    me, col = lax.axis_index("sp"), lax.axis_index("tp")
    rows, cols = stream_ref.shape
    half = rows // 2
    width = head_gain_ref.shape[1]
    key_width = width // 2
    f32 = jnp.float32
    meet, fold, across = fold_axes(me, col)
    loads = [
        pltpu.make_async_copy(a, b, load_sem.at[i])
        for i, (a, b) in enumerate(
            (
                (proj_hbm, proj),
                (sgate_hbm, sgate),
                (sup_hbm, sup),
                (gate_hbm, gate),
                (up_hbm, up),
                (sdown_hbm.at[col], sdown.at[0, 0]),
                (sdown_hbm.at[meet], sdown.at[0, 1]),
                (down_hbm.at[col], down.at[0, 0]),
                (down_hbm.at[meet], down.at[0, 1]),
            )
        )
    ]
    for load in loads:
        load.start()
    side = [flip(col, jnp.int32(j), 4) for j in range(4)]
    peer = lambda k: (flip(me, k, count), col)
    near_x, near_y = (me, side[1]), (me, side[2])
    friends = [peer(jnp.int32(k)) for k in range(1, count)] + [near_x, near_y]
    barrier = pltpu.get_barrier_semaphore()
    for device in friends:
        pl.semaphore_signal(barrier, inc=1, device_id=device, device_id_type=MESH_ID)
    for h in range(count):
        cut = slice(h * width, (h + 1) * width)
        pack[h, :rows, :] = jnp.concatenate([q_ref[:, cut], k_ref[:, cut]], axis=1)
        pack[h, rows:, :] = jnp.concatenate([v_ref[:half, cut], v_ref[half:, cut]], axis=1)
    pl.semaphore_wait(barrier, len(friends))

    def direct(buf, row, index):
        own = buf.at[(0,) + index]
        return (
            remote(own, buf.at[(1,) + index], gsend.at[row, 0], grecv.at[row, 0], near_x),
            remote(own, buf.at[(2,) + index], gsend.at[row, 1], grecv.at[row, 1], near_y),
        )

    def relays(buf, row, index):
        middle = buf.shape[-2] // 2
        top, low = pl.ds(0, middle), pl.ds(middle, middle)
        return (
            remote(
                buf.at[(1,) + index + (top,)], buf.at[(3,) + index + (top,)],
                gsend.at[row, 2], grecv.at[row, 2], near_y,
            ),
            remote(
                buf.at[(2,) + index + (low,)], buf.at[(3,) + index + (low,)],
                gsend.at[row, 3], grecv.at[row, 3], near_x,
            ),
        )

    def offer(buf, row, index=()):
        for copy in direct(buf, row, index):
            copy.start()

    def pass_on(buf, row, index=()):
        for first, second in zip(direct(buf, row, index), relays(buf, row, index)):
            first.wait_recv()
            second.start()

    def finish(buf, row, index=()):
        for copy in relays(buf, row, index):
            copy.wait_recv()

    def drain(buf, row, index=()):
        for copy in direct(buf, row, index) + relays(buf, row, index):
            copy.wait_send()

    def join(buf, row, index=()):
        own, other = buf.at[(0,) + index], buf.at[(1,) + index]
        return remote(own, other, fsend.at[row, 0], frecv.at[row, 0], (me, meet))

    def hand_over(buf, row, index=()):
        own, other = buf.at[(0,) + index], buf.at[(1,) + index]
        return remote(own, other, fsend.at[row, 1], frecv.at[row, 1], (me, fold))

    row_head, row_hidden, row_shared = count, count + count // 2, count

    def exchange(k):
        there = peer(k)
        return (
            remote(doc_ref, docs.at[me], xsend.at[0, k], xrecv.at[0, k], there),
            remote(pack.at[there[0]], qkv.at[me], xsend.at[1, k], xrecv.at[1, k], there),
        )

    def head_copy(k):
        there = peer(k)
        return remote(head_out.at[there[0]], held.at[me], hsend.at[k], hrecv.at[k], there)

    swaps = [
        remote(src.at[quarter], dst.at[1, i], wsend.at[j, i], wrecv.at[j, i], (me, fold))
        for j, (src, dst) in enumerate(((down_hbm, down), (sdown_hbm, sdown)))
        for i, quarter in enumerate((fold, across))
    ]
    for k in range(1, count):
        for copy in exchange(jnp.int32(k)):
            copy.start()
    for swap in swaps:
        swap.start()
    qkv[me] = pack[me]
    docs[me] = doc_ref[...]
    best_ref[...] = jnp.full(best_ref.shape, floor_score, f32)
    denom_ref[...] = jnp.zeros(denom_ref.shape, f32)
    numer_ref[...] = jnp.zeros(numer_ref.shape, f32)

    near = routes_ref[...] ^ me
    lane = lax.broadcasted_iota(jnp.int32, (128, rows), 0)
    hits = [near[j : j + 1, :] == lane for j in range(2)]
    present = hits[0] | hits[1]
    before = (
        lax.broadcasted_iota(jnp.int32, (rows, rows), 0)
        < lax.broadcasted_iota(jnp.int32, (rows, rows), 1)
    )
    place = jnp.dot(
        present.astype(f32).astype(jnp.bfloat16),
        before.astype(f32).astype(jnp.bfloat16),
        preferred_element_type=f32,
    )
    place = jnp.where(present, place, -1.0)
    slot = lax.broadcasted_iota(jnp.int32, (capacity, rows), 0).astype(f32)
    for k in range(count):
        onehot[k] = (slot == place[k : k + 1, :]).astype(f32).astype(jnp.bfloat16)
    portion = jnp.where(hits[0], weight_ref[0:1, :], 0.0) + jnp.where(
        hits[1], weight_ref[1:2, :], 0.0
    )
    portions[...] = jnp.transpose(portion)

    weight = lam_ref[me]
    gains = jnp.concatenate([head_gain_ref[...], head_gain_ref[...]], axis=1)
    factor = scaling * math.log2(math.e)
    lanes = lax.broadcasted_iota(jnp.int32, (rows, 2 * width), 1)

    def conclude(k):
        b = flip(me, k, count)
        heard = []
        for m in range(2):
            bests = [best_ref[b, pl.ds(2 * part + m, 1), :] for part in range(2)]
            top = jnp.maximum(*bests)
            fades = [jnp.exp2(best - top) for best in bests]
            denom, numer = [
                first * fades[0] + second * fades[1]
                for first, second in (
                    [denom_ref[b, pl.ds(2 * part + m, 1), :] for part in range(2)],
                    [numer_ref[b, 2 * part + m] for part in range(2)],
                )
            ]
            heard.append(numer / denom)
        contrast = heard[0] - weight * heard[1]
        contrast = contrast * lax.rsqrt(
            jnp.mean(contrast * contrast, axis=0, keepdims=True) + epsilon
        )
        stacked = jnp.concatenate([contrast[:, :half], contrast[:, half:]], axis=0)
        head_out[b] = (jnp.transpose(stacked) * gains).astype(jnp.bfloat16)

        @pl.when(k > 0)
        def _():
            head_copy(k).start()

    layer_of = lax.div(me, 2)
    lower = me < count // 2

    @pl.loop(0, count)
    def _(i):
        j = flip(me, i, count)

        @pl.when(i > 0)
        def _():
            for copy in exchange(i):
                copy.wait_recv()

        values = jnp.transpose(qkv[j, rows:, :].astype(f32)).astype(jnp.bfloat16)
        turned[j] = jnp.concatenate([values[:width], values[width:]], axis=1)
        moved = pltpu.roll(qkv[j, :rows, :].astype(f32), width, 1)
        for m in range(2):
            begin = width + m * key_width
            inside = (lanes >= begin) & (lanes < begin + key_width)
            queries[j, m] = jnp.where(inside, moved, 0.0).astype(jnp.bfloat16)
        doc_cols[j] = jnp.transpose(jnp.broadcast_to(docs[j].astype(f32), (8, rows)))

        def pair_of_tiles(step, carried):
            step = lax.div(i, 2) - step
            ahead = lax.broadcasted_iota(jnp.int32, (rows, rows), 0) - lax.broadcasted_iota(
                jnp.int32, (rows, rows), 1
            )
            tiles = []
            for part in range(2):
                second = 2 * step + part
                other = flip(me, jnp.minimum(second, i), count)
                q, k = jnp.maximum(j, other), jnp.minimum(j, other)
                limit = jnp.where(second <= i, (q - k) * rows, -rows)
                allowed = (ahead <= limit) & (doc_cols[k][:, 0:1] == docs[q].astype(f32))
                tiles.append((q, k, allowed))
            scores = [
                [
                    jnp.where(
                        allowed,
                        lax.dot_general(
                            qkv[k, :rows, :], queries[q, m], (((1,), (1,)), ((), ())),
                            preferred_element_type=f32,
                        )
                        * factor,
                        floor_score,
                    )
                    for m in range(2)
                ]
                for q, k, allowed in tiles
            ]
            for part, (q, k, _) in enumerate(tiles):
                for m in range(2):
                    row = pl.ds(2 * part + m, 1)
                    tile = scores[part][m]
                    best = best_ref[q, row, :]
                    new_best = jnp.maximum(best, jnp.max(tile, axis=0, keepdims=True))
                    fade = jnp.exp2(best - new_best)
                    weights = jnp.exp2(tile - new_best)
                    best_ref[q, row, :] = new_best
                    denom_ref[q, row, :] = denom_ref[q, row, :] * fade + jnp.sum(
                        weights, axis=0, keepdims=True
                    )
                    numer_ref[q, 2 * part + m] = numer_ref[q, 2 * part + m] * fade + jnp.dot(
                        turned[k], weights.astype(jnp.bfloat16), preferred_element_type=f32
                    )
            return carried

        pairs = lax.div(i, 2) + 1
        early = jnp.where(i == count - 1, count // 4, pairs)
        lax.fori_loop(0, early, pair_of_tiles, 0)

        @pl.when(i == count - 1)
        def _():
            @pl.loop(count // 2, count)
            def _(n):
                @pl.when((n < count - 1) | jnp.logical_not(lower))
                def _():
                    conclude(n)

        lax.fori_loop(early, pairs, pair_of_tiles, 0)

    @pl.when(lower)
    def _():
        conclude(jnp.int32(count - 1))

    @pl.loop(0, count // 2)
    def _(n):
        conclude(count // 2 - 1 - n)

    held[me] = head_out[me]
    @pl.loop(0, count // 2)
    def _(q):
        for k in range(2):
            @pl.when(2 * q + k > 0)
            def _():
                head_copy(2 * q + k).wait_recv()

        pair = flip(layer_of, q, count // 2)
        first, second = held[2 * pair], held[2 * pair + 1]
        for h in range(2):
            part = slice(h * width, (h + 1) * width)
            span = slice(h * half, (h + 1) * half)
            head_buf[0, q, span, :] = jnp.concatenate([first[:, part], second[:, part]], axis=1)
        offer(head_buf, row_head + q, (q,))

        @pl.when(q > 0)
        def _():
            pass_on(head_buf, row_head + q - 1, (q - 1,))

    pass_on(head_buf, row_head + count // 2 - 1, (count // 2 - 1,))
    loads[0].wait()

    def projected(j):
        blocks = [head_buf[j, flip(layer_of, jnp.int32(p), count // 2)] for p in range(count // 2)]
        block = jnp.concatenate(blocks, axis=1)
        return jnp.dot(block, proj[side[j]], preferred_element_type=f32)

    total = projected(0) + projected(1) + projected(2)
    for q in range(count // 2):
        finish(head_buf, row_head + q, (q,))
    total = total + projected(3)
    for h in range(2):
        span = slice(h * half, (h + 1) * half)
        hidden_buf[0, h] = (stream_ref[span, :].astype(f32) + total[span]).astype(jnp.bfloat16)
        offer(hidden_buf, row_hidden + h, (h,))

    def dispatch_far(k):
        return remote(outgoing.at[0, k], rows_in.at[0, k], zsend.at[k], zrecv.at[k], peer(k))

    def dispatch_near(k):
        return remote(outgoing.at[:, k], rows_in.at[:, k], zsend.at[k], zrecv.at[k], peer(k))

    def chosen(k, j):
        block = hidden_buf[j].reshape(rows, cols)
        return jnp.dot(onehot[k], block, preferred_element_type=f32).astype(jnp.bfloat16)

    for k in range(4, count):
        outgoing[0, k] = chosen(k, 0)
        dispatch_far(jnp.int32(k)).start()
    for h in range(2):
        pass_on(hidden_buf, row_hidden + h, (h,))

    def scaled(blocks):
        wide = [block.astype(f32) for block in blocks]
        squares = wide[0] * wide[0]
        for block in wide[1:]:
            squares = squares + block * block
        scale = lax.rsqrt(jnp.sum(squares, axis=1, keepdims=True) / (4 * cols) + epsilon)
        return [
            (block * scale * gain_ref[side[j]]).astype(jnp.bfloat16)
            for j, block in enumerate(wide)
        ]

    def gated_pair(blocks, first, second):
        gated, lifted = [
            sum(jnp.dot(block, w[side[j]], preferred_element_type=f32) for j, block in enumerate(blocks))
            for w in (first, second)
        ]
        return (jax.nn.silu(gated) * lifted).astype(jnp.bfloat16)

    for h in range(2):
        finish(hidden_buf, row_hidden + h, (h,))
    for j in range(4):
        outgoing[j, 1] = chosen(1, j)
    dispatch_near(jnp.int32(1)).start()
    for j in range(4):
        rows_in[j, 0] = chosen(0, j)
    for load in loads[1:]:
        load.wait()

    def first_half(k):
        acts[0, k] = gated_pair(scaled([rows_in[j, k] for j in range(4)]), gate, up)
        join(acts, k, (k,)).start()

    first_half(0)
    for h in range(2):
        span = slice(h * half, (h + 1) * half)
        for j, block in enumerate(scaled([hidden_buf[j, h] for j in range(4)])):
            normed[j, span, :] = block
    dispatch_near(jnp.int32(1)).wait_recv()
    for swap in swaps:
        swap.wait_recv()
    dispatch_far(jnp.int32(4)).wait_recv()
    offer(rows_in, 4, (4,))

    def give_back(k):
        return remote(made.at[k], back.at[k], rsend.at[k], rrecv.at[k], peer(k))

    far = list(range(4, count))
    after2, after3 = count - 4 - 2, count - 4 - 1
    sequence = [0, 1] + far[:after2] + [2] + far[after2:after3] + [3] + far[after3:]

    def turn(p):
        return sum(jnp.where(p == n, k, 0) for n, k in enumerate(sequence))

    def second_half(buf, second, index=()):
        return [
            jnp.dot(buf[(0,) + index], second[c, 0], preferred_element_type=f32)
            + jnp.dot(buf[(1,) + index], second[c, 1], preferred_element_type=f32)
            for c in range(2)
        ]

    def scattered(k, block):
        picked = lax.dot_general(
            onehot[k], block, (((0,), (0,)), ((), ())), preferred_element_type=f32
        )
        return portions[:, k : k + 1] * picked

    @pl.loop(0, count + 1)
    def _(i):
        @pl.when(i < 2)
        def _():
            for j in range(4):
                block = hidden_buf[j].reshape(rows, cols)
                outgoing[j, i + 2] = jnp.dot(
                    onehot[i + 2], block, preferred_element_type=f32
                ).astype(jnp.bfloat16)
            dispatch_near(i + 2).start()

        @pl.when(i < count - 5)
        def _():
            dispatch_far(i + 5).wait_recv()
            offer(rows_in, i + 5, (i + 5,))

        @pl.when(i < count - 4)
        def _():
            pass_on(rows_in, i + 4, (i + 4,))

        coming = turn(i + 1)

        @pl.when((i < count - 1) & (coming >= 4))
        def _():
            finish(rows_in, coming, (coming,))

        @pl.when((i < count - 1) & ((coming == 2) | (coming == 3)))
        def _():
            dispatch_near(coming).wait_recv()

        @pl.when(i < count - 1)
        def _():
            first_half(turn(i + 1))

        @pl.when(i == 0)
        def _():
            join(acts, 0, (0,)).wait_recv()
            for c, block in enumerate(second_half(acts, down, (0,))):
                made_two[c] = block.astype(jnp.bfloat16)

        @pl.when(i == 3)
        def _():
            shared_buf[0] = gated_pair([normed[j] for j in range(4)], sgate, sup)
            join(shared_buf, row_shared).start()

        @pl.when(i == 5)
        def _():
            join(shared_buf, row_shared).wait_recv()
            for c, block in enumerate(second_half(shared_buf, sdown)):
                shared_cols[c] = block

        @pl.when((i >= 1) & (i < count))
        def _():
            k = turn(i)
            join(acts, k, (k,)).wait_recv()
            own, other = second_half(acts, down, (k,))
            parts[0, k] = other.astype(jnp.bfloat16)
            hand_over(parts, k, (k,)).start()
            kept[k] = own

        @pl.when(i == 6)
        def _():
            for c in range(2):
                shared_cols[c] = shared_cols[c] + scattered(0, made_two[c])
            shared_part[0] = shared_cols[1].astype(jnp.bfloat16)

        @pl.when(i == count - 1)
        def _():
            hand_over(shared_part, row_shared).start()

        @pl.when(i >= 2)
        def _():
            k = turn(i - 1)
            hand_over(parts, k, (k,)).wait_recv()
            made[k] = (kept[k] + parts[1, k].astype(f32)).astype(jnp.bfloat16)
            give_back(k).start()

    total = shared_cols[0]
    for k in sequence[1:]:
        give_back(jnp.int32(k)).wait_recv()
        total = total + scattered(k, back[k])
    hand_over(shared_part, row_shared).wait_recv()
    total = total + shared_part[1].astype(f32)
    for h in range(2):
        span = slice(h * half, (h + 1) * half)
        out_ref[span, :] = (hidden_buf[0, h].astype(f32) + total[span]).astype(jnp.bfloat16)

    for swap in swaps:
        swap.wait_send()
    for q in range(count // 2):
        drain(head_buf, row_head + q, (q,))
    for h in range(2):
        drain(hidden_buf, row_hidden + h, (h,))
    join(shared_buf, row_shared).wait_send()
    hand_over(shared_part, row_shared).wait_send()

    @pl.loop(4, count)
    def _(k):
        drain(rows_in, k, (k,))
        dispatch_far(k).wait_send()

    @pl.loop(1, 4)
    def _(k):
        dispatch_near(k).wait_send()

    @pl.loop(1, count)
    def _(k):
        head_copy(k).wait_send()
        for copy in exchange(k):
            copy.wait_send()

    @pl.loop(0, count)
    def _(k):
        join(acts, k, (k,)).wait_send()

        @pl.when(k > 0)
        def _():
            hand_over(parts, k, (k,)).wait_send()
            give_back(k).wait_send()


def head_per_device(
    query_pairs,
    key_pairs,
    value_rows,
    doc_ids,
    contrast_lambda,
    head_gain,
    stream,
    out_proj,
    norm_gain,
    routes,
    route_weights,
    expert_gate,
    expert_up,
    expert_down,
    shared_gate,
    shared_up,
    shared_down,
):
    rows, cols = stream.shape
    count, sides = lax.axis_size("sp"), lax.axis_size("tp")
    width = value_rows.shape[1] // count
    capacity = 2 * rows * routes.shape[1] // count
    bf16, f32 = jnp.bfloat16, jnp.float32
    dma = pltpu.SemaphoreType.DMA
    split = lambda weight: weight.reshape(sides, weight.shape[-2] // sides, weight.shape[-1])
    down, sdown = split(expert_down[0]), split(shared_down)
    weight_shape = (sides, cols, cols)
    slots = (count, capacity, cols)
    return pl.pallas_call(
        functools.partial(layer_kernel, count, capacity, (width // 2) ** (-0.5)),
        out_shape=jax.ShapeDtypeStruct((rows, cols), bf16),
        in_specs=[SMEM] + [VMEM] * 9 + [ANY] * 7,
        out_specs=VMEM,
        scratch_shapes=[
            pltpu.VMEM((count, rows + rows // 2, 2 * width), bf16),
            pltpu.VMEM((count, rows + rows // 2, 2 * width), bf16),
            pltpu.VMEM((count, 1, rows), jnp.int32),
            pltpu.VMEM((count, rows, 8), f32),
            pltpu.VMEM((count, 2, rows, 2 * width), bf16),
            pltpu.VMEM((count, width, rows), bf16),
            pltpu.VMEM((count, 4, rows), f32),
            pltpu.VMEM((count, 4, rows), f32),
            pltpu.VMEM((count, 4, width, rows), f32),
            pltpu.VMEM((count, rows // 2, 2 * width), bf16),
            pltpu.VMEM((rows, 128), f32),
        ]
        + [pltpu.VMEM(weight_shape, bf16)] * 5
        + [pltpu.VMEM((2, 2, cols, cols), bf16)] * 2
        + [
            pltpu.VMEM((count, rows // 2, 2 * width), bf16),
            pltpu.VMEM((sides, count // 2, rows, cols // (count // 2)), bf16),
            pltpu.VMEM((sides, 2, rows // 2, cols), bf16),
            pltpu.VMEM((sides, rows, cols), bf16),
            pltpu.VMEM((2, rows, cols), bf16),
            pltpu.VMEM((2, rows, cols), bf16),
            pltpu.VMEM((count, capacity, rows), bf16),
            pltpu.VMEM((sides,) + slots, bf16),
            pltpu.VMEM((sides,) + slots, bf16),
            pltpu.VMEM((2,) + slots, bf16),
            pltpu.VMEM((2,) + slots, bf16),
            pltpu.VMEM(slots, f32),
            pltpu.VMEM(slots, bf16),
            pltpu.VMEM(slots, bf16),
            pltpu.VMEM((2, capacity, cols), bf16),
            pltpu.VMEM((2, rows, cols), f32),
            dma((9,)),
            dma((2, count)),
            dma((2, count)),
            dma((2, 2)),
            dma((2, 2)),
            dma((count,)),
            dma((count,)),
            dma((count + count // 2 + 2, 4)),
            dma((count + count // 2 + 2, 4)),
            dma((count + 1, 2)),
            dma((count + 1, 2)),
            dma((count,)),
            dma((count,)),
            dma((count,)),
            dma((count,)),
        ],
        compiler_params=pltpu.CompilerParams(
            collective_id=0, has_side_effects=True, vmem_limit_bytes=60 * 2**20
        ),
        name="layer",
    )(
        contrast_lambda,
        query_pairs,
        key_pairs,
        value_rows,
        doc_ids.reshape(1, rows),
        head_gain.reshape(1, width),
        stream,
        norm_gain.reshape(sides, 1, cols),
        routes.T,
        route_weights.T,
        split(out_proj),
        split(shared_gate),
        split(shared_up),
        split(expert_gate[0]),
        split(expert_up[0]),
        sdown,
        down,
    )


def choose(*args):
    query_pairs, value_rows, heads, stream = args[0], args[2], args[4].shape[0], args[6]
    count, sides = lax.axis_size("sp"), lax.axis_size("tp")
    width = value_rows.shape[1] // heads
    rows, cols = stream.shape
    hidden = {args[i].shape[-1] for i in (7, 11, 12, 13, 14, 15, 16)}
    fits = (
        heads == count
        and count & (count - 1) == 0
        and 8 <= count <= 128
        and sides == 4
        and 2 * width == 128
        and query_pairs.shape[1] == value_rows.shape[1] == cols
        and hidden == {cols}
        and all(args[i].shape[-2] == sides * cols for i in (7, 11, 12, 13, 14, 15, 16))
        and rows % 256 == 0
        and (2 * rows * args[9].shape[1]) % (128 * count) == 0
        and args[9].shape[1] == 2
    )
    return (head_per_device if fits else shards)(*args)


def solution(mesh):
    return jax.shard_map(
        choose,
        mesh=mesh,
        in_specs=(
            P("sp", "tp"),
            P("sp", "tp"),
            P("sp", "tp"),
            P("sp"),
            P("tp"),
            P(),
            P("sp", "tp"),
            P(None, "tp"),
            P(),
            P("sp", None),
            P("sp", None),
            P("sp", None, "tp"),
            P("sp", None, "tp"),
            P("sp", None, "tp"),
            P(None, "tp"),
            P(None, "tp"),
            P(None, "tp"),
        ),
        out_specs=P("sp", "tp"),
        check_vma=False,
    )
```

```python
import functools
import math

import jax
import jax.numpy as jnp
from jax import lax
from jax.experimental import pallas as pl
from jax.experimental.pallas import tpu as pltpu
from jax.sharding import PartitionSpec as P

epsilon = 1e-06
floor_score = -1e30


def add_columns(weight_rows, part_block):
    return jnp.dot(part_block, weight_rows, preferred_element_type=jnp.float32)


def shards(
    query_pairs,
    key_pairs,
    value_rows,
    doc_ids,
    contrast_lambda,
    head_gain,
    stream,
    out_proj,
    norm_gain,
    routes,
    route_weights,
    expert_gate,
    expert_up,
    expert_down,
    shared_gate,
    shared_up,
    shared_down,
):
    row_count = query_pairs.shape[0]
    local_heads = contrast_lambda.shape[0]
    key_width = query_pairs.shape[1] // (2 * local_heads)
    value_width = value_rows.shape[1] // local_heads
    scaling = key_width ** (-0.5)
    first_row = lax.axis_index("sp") * row_count
    query_pos = first_row + jnp.arange(row_count, dtype=jnp.int32)
    last_query = first_row + row_count - 1
    first_doc = doc_ids[0]
    query_split = query_pairs.reshape(row_count, local_heads, 2, key_width)

    def absorb_block(running, key_block, value_block, doc_block, key_start):
        best, denom, numer = running
        span_len = key_block.shape[0]
        key_pos = key_start + jnp.arange(span_len, dtype=jnp.int32)
        allowed = (key_pos[None, :] <= query_pos[:, None]) & (
            doc_block[None, :] == doc_ids[:, None]
        )
        scores = (
            jnp.einsum(
                "qhmd,khmd->hmqk",
                query_split,
                key_block.reshape(span_len, local_heads, 2, key_width),
                preferred_element_type=jnp.float32,
            )
            * scaling
        )
        scores = jnp.where(allowed, scores, floor_score)
        new_best = jnp.maximum(best, jnp.max(scores, axis=-1))
        weights = jnp.where(allowed, jnp.exp(scores - new_best[..., None]), 0.0)
        fade = jnp.exp(best - new_best)
        denom = denom * fade + jnp.sum(weights, axis=-1)
        numer = numer * fade[..., None] + jnp.einsum(
            "hmqk,khv->hmqv",
            weights.astype(jnp.bfloat16),
            value_block.reshape(span_len, local_heads, value_width),
            preferred_element_type=jnp.float32,
        )
        return (new_best, denom, numer)

    start_best = jnp.full((local_heads, 2, row_count), floor_score, jnp.float32)
    start_denom = jnp.zeros((local_heads, 2, row_count), jnp.float32)
    start_numer = jnp.zeros((local_heads, 2, row_count, value_width), jnp.float32)
    key_piece = lax.all_gather(key_pairs, "sp", axis=0, tiled=True)
    value_piece = lax.all_gather(value_rows, "sp", axis=0, tiled=True)
    doc_piece = lax.all_gather(doc_ids, "sp", axis=0, tiled=True)
    length = key_piece.shape[0]
    span_len = row_count * max(1, 512 // row_count)

    def one_span(span_index, carried):
        offset = span_index * span_len
        key_block = lax.dynamic_slice_in_dim(key_piece, offset, span_len, 0)
        value_block = lax.dynamic_slice_in_dim(value_piece, offset, span_len, 0)
        doc_block = lax.dynamic_slice_in_dim(doc_piece, offset, span_len, 0)
        needed = (offset <= last_query) & (doc_block[span_len - 1] >= first_doc)
        return lax.cond(
            needed,
            lambda held: absorb_block(held, key_block, value_block, doc_block, offset),
            lambda held: held,
            carried,
        )

    best, denom, numer = lax.fori_loop(
        0, length // span_len, one_span, (start_best, start_denom, start_numer)
    )
    heard = numer / denom[..., None]
    contrast = heard[:, 0] - contrast_lambda[:, None, None] * heard[:, 1]
    contrast = (
        contrast
        * lax.rsqrt(jnp.mean(contrast * contrast, axis=-1, keepdims=True) + epsilon)
        * head_gain
    )
    head_out = (
        jnp.transpose(contrast, (1, 0, 2))
        .reshape(row_count, local_heads * value_width)
        .astype(jnp.bfloat16)
    )
    projected = add_columns(out_proj, lax.all_gather(head_out, "tp", axis=1, tiled=True))
    hidden_cols = (stream.astype(jnp.float32) + projected).astype(jnp.bfloat16)
    hidden_rows = lax.all_gather(hidden_cols, "tp", axis=1, tiled=True)
    widened = hidden_rows.astype(jnp.float32)
    normed = (
        widened
        * lax.rsqrt(jnp.mean(widened * widened, axis=-1, keepdims=True) + epsilon)
        * norm_gain
    ).astype(jnp.bfloat16)
    shared_act = (
        jax.nn.silu(jnp.dot(normed, shared_gate, preferred_element_type=jnp.float32))
        * jnp.dot(normed, shared_up, preferred_element_type=jnp.float32)
    ).astype(jnp.bfloat16)
    shared_cols = add_columns(shared_down, lax.all_gather(shared_act, "tp", axis=1, tiled=True))
    expert_count = lax.axis_size("sp")
    route_count = routes.shape[1]
    capacity = 2 * row_count * route_count // expert_count
    flat_routes = routes.reshape(-1)
    hits = (flat_routes[:, None] == jnp.arange(expert_count, dtype=jnp.int32)[None, :]).astype(
        jnp.int32
    )
    position = jnp.sum(jnp.cumsum(hits, axis=0) * hits, axis=1) - 1
    target = flat_routes * capacity + position
    sources = jnp.arange(flat_routes.shape[0], dtype=jnp.int32) // route_count
    owner = jnp.zeros((expert_count * capacity,), jnp.int32).at[target].set(sources)
    outgoing = normed[owner].reshape(expert_count, capacity, normed.shape[1])
    gate_cols = expert_gate[0]
    up_cols = expert_up[0]
    down_cols = expert_down[0]
    slice_width = outgoing.shape[2] // lax.axis_size("tp")
    own_slice = lax.dynamic_slice_in_dim(
        outgoing, lax.axis_index("tp") * slice_width, slice_width, 2
    )
    arrived = lax.all_to_all(own_slice, "sp", split_axis=0, concat_axis=0, tiled=True)
    apply_arrived = lax.all_gather(arrived, "tp", axis=2, tiled=True)
    gated = jnp.einsum("snd,df->snf", apply_arrived, gate_cols, preferred_element_type=jnp.float32)
    lifted = jnp.einsum("snd,df->snf", apply_arrived, up_cols, preferred_element_type=jnp.float32)
    expert_act = (jax.nn.silu(gated) * lifted).astype(jnp.bfloat16)
    expert_out = add_columns(
        down_cols, lax.all_gather(expert_act, "tp", axis=2, tiled=True)
    ).astype(jnp.bfloat16)
    returned = lax.all_to_all(expert_out, "sp", split_axis=0, concat_axis=0, tiled=True)
    flat_back = returned.reshape(expert_count * capacity, returned.shape[2])
    picked = (
        flat_back[target].reshape(row_count, route_count, returned.shape[2]).astype(jnp.float32)
    )
    routed = jnp.sum(picked * route_weights[:, :, None], axis=1)
    return (hidden_cols.astype(jnp.float32) + shared_cols + routed).astype(jnp.bfloat16)


MESH_ID = pl.DeviceIdType.MESH
VMEM = pl.BlockSpec(memory_space=pltpu.VMEM)
ANY = pl.BlockSpec(memory_space=pl.ANY)
SMEM = pl.BlockSpec(memory_space=pltpu.SMEM)


def flip(index, mask, size):
    out, bit = 0, 1
    while bit < size:
        out = out + bit * lax.rem(lax.div(index, bit) + lax.div(mask, bit), 2)
        bit *= 2
    return out


def remote(src, dst, send, recv, device):
    return pltpu.make_async_remote_copy(
        src_ref=src,
        dst_ref=dst,
        send_sem=send,
        recv_sem=recv,
        device_id=device,
        device_id_type=MESH_ID,
    )


def fold_axes(me, col):
    core = lax.rem(me, 2)
    return flip(col, 2 - core, 4), flip(col, 1 + core, 4), flip(col, jnp.int32(3), 4)


def layer_kernel(
    count,
    capacity,
    scaling,
    lam_ref,
    q_ref,
    k_ref,
    v_ref,
    doc_ref,
    head_gain_ref,
    stream_ref,
    gain_ref,
    routes_ref,
    weight_ref,
    proj_hbm,
    sgate_hbm,
    sup_hbm,
    gate_hbm,
    up_hbm,
    sdown_hbm,
    down_hbm,
    out_ref,
    pack,
    qkv,
    docs,
    doc_cols,
    queries,
    turned,
    best_ref,
    denom_ref,
    numer_ref,
    head_out,
    portions,
    proj,
    sgate,
    sup,
    gate,
    up,
    sdown,
    down,
    held,
    head_buf,
    hidden_buf,
    normed,
    shared_buf,
    shared_part,
    onehot,
    outgoing,
    rows_in,
    acts,
    parts,
    kept,
    made,
    back,
    made_two,
    shared_cols,
    load_sem,
    xsend,
    xrecv,
    wsend,
    wrecv,
    hsend,
    hrecv,
    gsend,
    grecv,
    fsend,
    frecv,
    zsend,
    zrecv,
    rsend,
    rrecv,
):
    me, col = lax.axis_index("sp"), lax.axis_index("tp")
    rows, cols = stream_ref.shape
    half = rows // 2
    width = head_gain_ref.shape[1]
    key_width = width // 2
    f32 = jnp.float32
    meet, fold, across = fold_axes(me, col)
    loads = [
        pltpu.make_async_copy(a, b, load_sem.at[i])
        for i, (a, b) in enumerate(
            (
                (proj_hbm, proj),
                (sgate_hbm, sgate),
                (sup_hbm, sup),
                (gate_hbm, gate),
                (up_hbm, up),
                (sdown_hbm.at[col], sdown.at[0, 0]),
                (sdown_hbm.at[meet], sdown.at[0, 1]),
                (down_hbm.at[col], down.at[0, 0]),
                (down_hbm.at[meet], down.at[0, 1]),
            )
        )
    ]
    for load in loads:
        load.start()
    side = [flip(col, jnp.int32(j), 4) for j in range(4)]
    peer = lambda k: (flip(me, k, count), col)
    near_x, near_y = (me, side[1]), (me, side[2])
    friends = [peer(jnp.int32(k)) for k in range(1, count)] + [near_x, near_y]
    barrier = pltpu.get_barrier_semaphore()
    for device in friends:
        pl.semaphore_signal(barrier, inc=1, device_id=device, device_id_type=MESH_ID)
    for h in range(count):
        cut = slice(h * width, (h + 1) * width)
        pack[h, :rows, :] = jnp.concatenate([q_ref[:, cut], k_ref[:, cut]], axis=1)
        pack[h, rows:, :] = jnp.concatenate([v_ref[:half, cut], v_ref[half:, cut]], axis=1)
    pl.semaphore_wait(barrier, len(friends))

    def direct(buf, row, index):
        own = buf.at[(0,) + index]
        return (
            remote(own, buf.at[(1,) + index], gsend.at[row, 0], grecv.at[row, 0], near_x),
            remote(own, buf.at[(2,) + index], gsend.at[row, 1], grecv.at[row, 1], near_y),
        )

    def relays(buf, row, index):
        middle = buf.shape[-2] // 2
        top, low = pl.ds(0, middle), pl.ds(middle, middle)
        return (
            remote(
                buf.at[(1,) + index + (top,)], buf.at[(3,) + index + (top,)],
                gsend.at[row, 2], grecv.at[row, 2], near_y,
            ),
            remote(
                buf.at[(2,) + index + (low,)], buf.at[(3,) + index + (low,)],
                gsend.at[row, 3], grecv.at[row, 3], near_x,
            ),
        )

    def offer(buf, row, index=()):
        for copy in direct(buf, row, index):
            copy.start()

    def pass_on(buf, row, index=()):
        for first, second in zip(direct(buf, row, index), relays(buf, row, index)):
            first.wait_recv()
            second.start()

    def finish(buf, row, index=()):
        for copy in relays(buf, row, index):
            copy.wait_recv()

    def drain(buf, row, index=()):
        for copy in direct(buf, row, index) + relays(buf, row, index):
            copy.wait_send()

    def join(buf, row, index=()):
        own, other = buf.at[(0,) + index], buf.at[(1,) + index]
        return remote(own, other, fsend.at[row, 0], frecv.at[row, 0], (me, meet))

    def hand_over(buf, row, index=()):
        own, other = buf.at[(0,) + index], buf.at[(1,) + index]
        return remote(own, other, fsend.at[row, 1], frecv.at[row, 1], (me, fold))

    row_head, row_hidden, row_shared = count, count + count // 2, count

    def exchange(k):
        there = peer(k)
        return (
            remote(doc_ref, docs.at[me], xsend.at[0, k], xrecv.at[0, k], there),
            remote(pack.at[there[0]], qkv.at[me], xsend.at[1, k], xrecv.at[1, k], there),
        )

    def head_copy(k):
        there = peer(k)
        return remote(head_out.at[there[0]], held.at[me], hsend.at[k], hrecv.at[k], there)

    swaps = [
        remote(src.at[quarter], dst.at[1, i], wsend.at[j, i], wrecv.at[j, i], (me, fold))
        for j, (src, dst) in enumerate(((down_hbm, down), (sdown_hbm, sdown)))
        for i, quarter in enumerate((fold, across))
    ]
    for k in range(1, count):
        for copy in exchange(jnp.int32(k)):
            copy.start()
    for swap in swaps:
        swap.start()
    qkv[me] = pack[me]
    docs[me] = doc_ref[...]
    best_ref[...] = jnp.full(best_ref.shape, floor_score, f32)
    denom_ref[...] = jnp.zeros(denom_ref.shape, f32)
    numer_ref[...] = jnp.zeros(numer_ref.shape, f32)

    near = routes_ref[...] ^ me
    lane = lax.broadcasted_iota(jnp.int32, (128, rows), 0)
    hits = [near[j : j + 1, :] == lane for j in range(2)]
    present = hits[0] | hits[1]
    before = (
        lax.broadcasted_iota(jnp.int32, (rows, rows), 0)
        < lax.broadcasted_iota(jnp.int32, (rows, rows), 1)
    )
    place = jnp.dot(
        present.astype(f32).astype(jnp.bfloat16),
        before.astype(f32).astype(jnp.bfloat16),
        preferred_element_type=f32,
    )
    place = jnp.where(present, place, -1.0)
    slot = lax.broadcasted_iota(jnp.int32, (capacity, rows), 0).astype(f32)
    for k in range(count):
        onehot[k] = (slot == place[k : k + 1, :]).astype(f32).astype(jnp.bfloat16)
    portion = jnp.where(hits[0], weight_ref[0:1, :], 0.0) + jnp.where(
        hits[1], weight_ref[1:2, :], 0.0
    )
    portions[...] = jnp.transpose(portion)

    weight = lam_ref[me]
    gains = jnp.concatenate([head_gain_ref[...], head_gain_ref[...]], axis=1)
    factor = scaling * math.log2(math.e)
    lanes = lax.broadcasted_iota(jnp.int32, (rows, 2 * width), 1)

    def conclude(k):
        b = flip(me, k, count)
        heard = []
        for m in range(2):
            bests = [best_ref[b, pl.ds(2 * part + m, 1), :] for part in range(2)]
            top = jnp.maximum(*bests)
            fades = [jnp.exp2(best - top) for best in bests]
            denom, numer = [
                first * fades[0] + second * fades[1]
                for first, second in (
                    [denom_ref[b, pl.ds(2 * part + m, 1), :] for part in range(2)],
                    [numer_ref[b, 2 * part + m] for part in range(2)],
                )
            ]
            heard.append(numer / denom)
        contrast = heard[0] - weight * heard[1]
        contrast = contrast * lax.rsqrt(
            jnp.mean(contrast * contrast, axis=0, keepdims=True) + epsilon
        )
        stacked = jnp.concatenate([contrast[:, :half], contrast[:, half:]], axis=0)
        head_out[b] = (jnp.transpose(stacked) * gains).astype(jnp.bfloat16)

        @pl.when(k > 0)
        def _():
            head_copy(k).start()

    layer_of = lax.div(me, 2)
    lower = me < count // 2

    @pl.loop(0, count)
    def _(i):
        j = flip(me, i, count)

        @pl.when(i > 0)
        def _():
            for copy in exchange(i):
                copy.wait_recv()

        values = jnp.transpose(qkv[j, rows:, :].astype(f32)).astype(jnp.bfloat16)
        turned[j] = jnp.concatenate([values[:width], values[width:]], axis=1)
        moved = pltpu.roll(qkv[j, :rows, :].astype(f32), width, 1)
        for m in range(2):
            begin = width + m * key_width
            inside = (lanes >= begin) & (lanes < begin + key_width)
            queries[j, m] = jnp.where(inside, moved, 0.0).astype(jnp.bfloat16)
        doc_cols[j] = jnp.transpose(jnp.broadcast_to(docs[j].astype(f32), (8, rows)))

        def pair_of_tiles(step, carried):
            step = lax.div(i, 2) - step
            ahead = lax.broadcasted_iota(jnp.int32, (rows, rows), 0) - lax.broadcasted_iota(
                jnp.int32, (rows, rows), 1
            )
            tiles = []
            for part in range(2):
                second = 2 * step + part
                other = flip(me, jnp.minimum(second, i), count)
                q, k = jnp.maximum(j, other), jnp.minimum(j, other)
                limit = jnp.where(second <= i, (q - k) * rows, -rows)
                allowed = (ahead <= limit) & (doc_cols[k][:, 0:1] == docs[q].astype(f32))
                tiles.append((q, k, allowed))
            scores = [
                [
                    jnp.where(
                        allowed,
                        lax.dot_general(
                            qkv[k, :rows, :], queries[q, m], (((1,), (1,)), ((), ())),
                            preferred_element_type=f32,
                        )
                        * factor,
                        floor_score,
                    )
                    for m in range(2)
                ]
                for q, k, allowed in tiles
            ]
            for part, (q, k, _) in enumerate(tiles):
                for m in range(2):
                    row = pl.ds(2 * part + m, 1)
                    tile = scores[part][m]
                    best = best_ref[q, row, :]
                    new_best = jnp.maximum(best, jnp.max(tile, axis=0, keepdims=True))
                    fade = jnp.exp2(best - new_best)
                    weights = jnp.exp2(tile - new_best)
                    best_ref[q, row, :] = new_best
                    denom_ref[q, row, :] = denom_ref[q, row, :] * fade + jnp.sum(
                        weights, axis=0, keepdims=True
                    )
                    numer_ref[q, 2 * part + m] = numer_ref[q, 2 * part + m] * fade + jnp.dot(
                        turned[k], weights.astype(jnp.bfloat16), preferred_element_type=f32
                    )
            return carried

        pairs = lax.div(i, 2) + 1
        early = jnp.where(i == count - 1, count // 4, pairs)
        lax.fori_loop(0, early, pair_of_tiles, 0)

        @pl.when(i == count - 1)
        def _():
            @pl.loop(count // 2, count)
            def _(n):
                @pl.when((n < count - 1) | jnp.logical_not(lower))
                def _():
                    conclude(n)

        lax.fori_loop(early, pairs, pair_of_tiles, 0)

    @pl.when(lower)
    def _():
        conclude(jnp.int32(count - 1))

    @pl.loop(0, count // 2)
    def _(n):
        conclude(count // 2 - 1 - n)

    held[me] = head_out[me]
    @pl.loop(0, count // 2)
    def _(q):
        for k in range(2):
            @pl.when(2 * q + k > 0)
            def _():
                head_copy(2 * q + k).wait_recv()

        pair = flip(layer_of, q, count // 2)
        first, second = held[2 * pair], held[2 * pair + 1]
        for h in range(2):
            part = slice(h * width, (h + 1) * width)
            span = slice(h * half, (h + 1) * half)
            head_buf[0, q, span, :] = jnp.concatenate([first[:, part], second[:, part]], axis=1)
        offer(head_buf, row_head + q, (q,))

        @pl.when(q > 0)
        def _():
            pass_on(head_buf, row_head + q - 1, (q - 1,))

    pass_on(head_buf, row_head + count // 2 - 1, (count // 2 - 1,))
    loads[0].wait()

    def projected(j):
        blocks = [head_buf[j, flip(layer_of, jnp.int32(p), count // 2)] for p in range(count // 2)]
        block = jnp.concatenate(blocks, axis=1)
        return jnp.dot(block, proj[side[j]], preferred_element_type=f32)

    total = projected(0) + projected(1) + projected(2)
    for q in range(count // 2):
        finish(head_buf, row_head + q, (q,))
    total = total + projected(3)
    for h in range(2):
        span = slice(h * half, (h + 1) * half)
        hidden_buf[0, h] = (stream_ref[span, :].astype(f32) + total[span]).astype(jnp.bfloat16)
        offer(hidden_buf, row_hidden + h, (h,))

    def dispatch_far(k):
        return remote(outgoing.at[0, k], rows_in.at[0, k], zsend.at[k], zrecv.at[k], peer(k))

    def dispatch_near(k):
        return remote(outgoing.at[:, k], rows_in.at[:, k], zsend.at[k], zrecv.at[k], peer(k))

    def chosen(k, j):
        block = hidden_buf[j].reshape(rows, cols)
        return jnp.dot(onehot[k], block, preferred_element_type=f32).astype(jnp.bfloat16)

    for k in range(4, count):
        outgoing[0, k] = chosen(k, 0)
        dispatch_far(jnp.int32(k)).start()
    for h in range(2):
        pass_on(hidden_buf, row_hidden + h, (h,))

    def scaled(blocks):
        wide = [block.astype(f32) for block in blocks]
        squares = wide[0] * wide[0]
        for block in wide[1:]:
            squares = squares + block * block
        scale = lax.rsqrt(jnp.sum(squares, axis=1, keepdims=True) / (4 * cols) + epsilon)
        return [
            (block * scale * gain_ref[side[j]]).astype(jnp.bfloat16)
            for j, block in enumerate(wide)
        ]

    def gated_pair(blocks, first, second):
        gated, lifted = [
            sum(jnp.dot(block, w[side[j]], preferred_element_type=f32) for j, block in enumerate(blocks))
            for w in (first, second)
        ]
        return (jax.nn.silu(gated) * lifted).astype(jnp.bfloat16)

    for h in range(2):
        finish(hidden_buf, row_hidden + h, (h,))
    for j in range(4):
        outgoing[j, 1] = chosen(1, j)
    dispatch_near(jnp.int32(1)).start()
    for j in range(4):
        rows_in[j, 0] = chosen(0, j)
    for load in loads[1:]:
        load.wait()

    def first_half(k):
        acts[0, k] = gated_pair(scaled([rows_in[j, k] for j in range(4)]), gate, up)
        join(acts, k, (k,)).start()

    first_half(0)
    dispatch_near(jnp.int32(1)).wait_recv()
    for swap in swaps:
        swap.wait_recv()
    first_half(1)
    dispatch_far(jnp.int32(4)).wait_recv()
    offer(rows_in, 4, (4,))

    def give_back(k):
        return remote(made.at[k], back.at[k], rsend.at[k], rrecv.at[k], peer(k))

    far = list(range(4, count))
    after2, after3 = count - 4 - 2, count - 4 - 1
    sequence = [0, 1] + far[:after2] + [2] + far[after2:after3] + [3] + far[after3:]

    def turn(p):
        return sum(jnp.where(p == n, k, 0) for n, k in enumerate(sequence))

    def second_half(buf, second, index=()):
        return [
            jnp.dot(buf[(0,) + index], second[c, 0], preferred_element_type=f32)
            + jnp.dot(buf[(1,) + index], second[c, 1], preferred_element_type=f32)
            for c in range(2)
        ]

    def scattered(k, block):
        picked = lax.dot_general(
            onehot[k], block, (((0,), (0,)), ((), ())), preferred_element_type=f32
        )
        return portions[:, k : k + 1] * picked

    @pl.loop(0, count + 1)
    def _(i):
        @pl.when(i < 2)
        def _():
            for j in range(4):
                block = hidden_buf[j].reshape(rows, cols)
                outgoing[j, i + 2] = jnp.dot(
                    onehot[i + 2], block, preferred_element_type=f32
                ).astype(jnp.bfloat16)
            dispatch_near(i + 2).start()

        @pl.when(i < count - 5)
        def _():
            dispatch_far(i + 5).wait_recv()
            offer(rows_in, i + 5, (i + 5,))

        @pl.when(i < count - 4)
        def _():
            pass_on(rows_in, i + 4, (i + 4,))

        coming = turn(i + 1)

        @pl.when((i < count - 1) & (coming >= 4))
        def _():
            finish(rows_in, coming, (coming,))

        @pl.when((i < count - 1) & ((coming == 2) | (coming == 3)))
        def _():
            dispatch_near(coming).wait_recv()

        @pl.when((i >= 1) & (i < count - 1))
        def _():
            first_half(coming)

        @pl.when(i == 0)
        def _():
            join(acts, 0, (0,)).wait_recv()
            for c, block in enumerate(second_half(acts, down, (0,))):
                made_two[c] = block.astype(jnp.bfloat16)

        @pl.when(i == 3)
        def _():
            for h in range(2):
                span = slice(h * half, (h + 1) * half)
                for j, block in enumerate(scaled([hidden_buf[j, h] for j in range(4)])):
                    normed[j, span, :] = block
            shared_buf[0] = gated_pair([normed[j] for j in range(4)], sgate, sup)
            join(shared_buf, row_shared).start()

        @pl.when(i == 5)
        def _():
            join(shared_buf, row_shared).wait_recv()
            for c, block in enumerate(second_half(shared_buf, sdown)):
                shared_cols[c] = block

        @pl.when((i >= 1) & (i < count))
        def _():
            k = turn(i)
            join(acts, k, (k,)).wait_recv()
            own, other = second_half(acts, down, (k,))
            parts[0, k] = other.astype(jnp.bfloat16)
            hand_over(parts, k, (k,)).start()
            kept[k] = own

        @pl.when(i == 6)
        def _():
            for c in range(2):
                shared_cols[c] = shared_cols[c] + scattered(0, made_two[c])
            shared_part[0] = shared_cols[1].astype(jnp.bfloat16)

        @pl.when(i == count - 1)
        def _():
            hand_over(shared_part, row_shared).start()

        @pl.when(i >= 2)
        def _():
            k = turn(i - 1)
            hand_over(parts, k, (k,)).wait_recv()
            made[k] = (kept[k] + parts[1, k].astype(f32)).astype(jnp.bfloat16)
            give_back(k).start()

    total = shared_cols[0]
    for k in sequence[1:]:
        give_back(jnp.int32(k)).wait_recv()
        total = total + scattered(k, back[k])
    hand_over(shared_part, row_shared).wait_recv()
    total = total + shared_part[1].astype(f32)
    for h in range(2):
        span = slice(h * half, (h + 1) * half)
        out_ref[span, :] = (hidden_buf[0, h].astype(f32) + total[span]).astype(jnp.bfloat16)

    for swap in swaps:
        swap.wait_send()
    for q in range(count // 2):
        drain(head_buf, row_head + q, (q,))
    for h in range(2):
        drain(hidden_buf, row_hidden + h, (h,))
    join(shared_buf, row_shared).wait_send()
    hand_over(shared_part, row_shared).wait_send()

    @pl.loop(4, count)
    def _(k):
        drain(rows_in, k, (k,))
        dispatch_far(k).wait_send()

    @pl.loop(1, 4)
    def _(k):
        dispatch_near(k).wait_send()

    @pl.loop(1, count)
    def _(k):
        head_copy(k).wait_send()
        for copy in exchange(k):
            copy.wait_send()

    @pl.loop(0, count)
    def _(k):
        join(acts, k, (k,)).wait_send()

        @pl.when(k > 0)
        def _():
            hand_over(parts, k, (k,)).wait_send()
            give_back(k).wait_send()


def head_per_device(
    query_pairs,
    key_pairs,
    value_rows,
    doc_ids,
    contrast_lambda,
    head_gain,
    stream,
    out_proj,
    norm_gain,
    routes,
    route_weights,
    expert_gate,
    expert_up,
    expert_down,
    shared_gate,
    shared_up,
    shared_down,
):
    rows, cols = stream.shape
    count, sides = lax.axis_size("sp"), lax.axis_size("tp")
    width = value_rows.shape[1] // count
    capacity = 2 * rows * routes.shape[1] // count
    bf16, f32 = jnp.bfloat16, jnp.float32
    dma = pltpu.SemaphoreType.DMA
    split = lambda weight: weight.reshape(sides, weight.shape[-2] // sides, weight.shape[-1])
    down, sdown = split(expert_down[0]), split(shared_down)
    weight_shape = (sides, cols, cols)
    slots = (count, capacity, cols)
    return pl.pallas_call(
        functools.partial(layer_kernel, count, capacity, (width // 2) ** (-0.5)),
        out_shape=jax.ShapeDtypeStruct((rows, cols), bf16),
        in_specs=[SMEM] + [VMEM] * 9 + [ANY] * 7,
        out_specs=VMEM,
        scratch_shapes=[
            pltpu.VMEM((count, rows + rows // 2, 2 * width), bf16),
            pltpu.VMEM((count, rows + rows // 2, 2 * width), bf16),
            pltpu.VMEM((count, 1, rows), jnp.int32),
            pltpu.VMEM((count, rows, 8), f32),
            pltpu.VMEM((count, 2, rows, 2 * width), bf16),
            pltpu.VMEM((count, width, rows), bf16),
            pltpu.VMEM((count, 4, rows), f32),
            pltpu.VMEM((count, 4, rows), f32),
            pltpu.VMEM((count, 4, width, rows), f32),
            pltpu.VMEM((count, rows // 2, 2 * width), bf16),
            pltpu.VMEM((rows, 128), f32),
        ]
        + [pltpu.VMEM(weight_shape, bf16)] * 5
        + [pltpu.VMEM((2, 2, cols, cols), bf16)] * 2
        + [
            pltpu.VMEM((count, rows // 2, 2 * width), bf16),
            pltpu.VMEM((sides, count // 2, rows, cols // (count // 2)), bf16),
            pltpu.VMEM((sides, 2, rows // 2, cols), bf16),
            pltpu.VMEM((sides, rows, cols), bf16),
            pltpu.VMEM((2, rows, cols), bf16),
            pltpu.VMEM((2, rows, cols), bf16),
            pltpu.VMEM((count, capacity, rows), bf16),
            pltpu.VMEM((sides,) + slots, bf16),
            pltpu.VMEM((sides,) + slots, bf16),
            pltpu.VMEM((2,) + slots, bf16),
            pltpu.VMEM((2,) + slots, bf16),
            pltpu.VMEM(slots, f32),
            pltpu.VMEM(slots, bf16),
            pltpu.VMEM(slots, bf16),
            pltpu.VMEM((2, capacity, cols), bf16),
            pltpu.VMEM((2, rows, cols), f32),
            dma((9,)),
            dma((2, count)),
            dma((2, count)),
            dma((2, 2)),
            dma((2, 2)),
            dma((count,)),
            dma((count,)),
            dma((count + count // 2 + 2, 4)),
            dma((count + count // 2 + 2, 4)),
            dma((count + 1, 2)),
            dma((count + 1, 2)),
            dma((count,)),
            dma((count,)),
            dma((count,)),
            dma((count,)),
        ],
        compiler_params=pltpu.CompilerParams(
            collective_id=0, has_side_effects=True, vmem_limit_bytes=60 * 2**20
        ),
        name="layer",
    )(
        contrast_lambda,
        query_pairs,
        key_pairs,
        value_rows,
        doc_ids.reshape(1, rows),
        head_gain.reshape(1, width),
        stream,
        norm_gain.reshape(sides, 1, cols),
        routes.T,
        route_weights.T,
        split(out_proj),
        split(shared_gate),
        split(shared_up),
        split(expert_gate[0]),
        split(expert_up[0]),
        sdown,
        down,
    )


def choose(*args):
    query_pairs, value_rows, heads, stream = args[0], args[2], args[4].shape[0], args[6]
    count, sides = lax.axis_size("sp"), lax.axis_size("tp")
    width = value_rows.shape[1] // heads
    rows, cols = stream.shape
    hidden = {args[i].shape[-1] for i in (7, 11, 12, 13, 14, 15, 16)}
    fits = (
        heads == count
        and count & (count - 1) == 0
        and 8 <= count <= 128
        and sides == 4
        and 2 * width == 128
        and query_pairs.shape[1] == value_rows.shape[1] == cols
        and hidden == {cols}
        and all(args[i].shape[-2] == sides * cols for i in (7, 11, 12, 13, 14, 15, 16))
        and rows % 256 == 0
        and (2 * rows * args[9].shape[1]) % (128 * count) == 0
        and args[9].shape[1] == 2
    )
    return (head_per_device if fits else shards)(*args)


def solution(mesh):
    return jax.shard_map(
        choose,
        mesh=mesh,
        in_specs=(
            P("sp", "tp"),
            P("sp", "tp"),
            P("sp", "tp"),
            P("sp"),
            P("tp"),
            P(),
            P("sp", "tp"),
            P(None, "tp"),
            P(),
            P("sp", None),
            P("sp", None),
            P("sp", None, "tp"),
            P("sp", None, "tp"),
            P("sp", None, "tp"),
            P(None, "tp"),
            P(None, "tp"),
            P(None, "tp"),
        ),
        out_specs=P("sp", "tp"),
        check_vma=False,
    )
```
